32 devices in a mesh: row: 8 (over z, core), col: 4 (over y, x).
Axes of the slice: x: 2, y: 2, z: 4, core: 2. Of those that a mesh axis runs over, the one named last changes fastest.
Arguments:
- mix_input: bfloat16 [4, 2048, 1024], P('col', 'row'), may hold values from -6 to 6
- gate_logits: bfloat16 [4, 2048, 2048], P('col', 'row'), may hold values from -8 to 8
- w_proj: bfloat16 [1024, 2048], P('col'), may hold values from -0.1875 to 0.1875
Outputs:
- mixed: bfloat16 [4, 2048, 2048], P('col', 'row')
The draws below stay inside these ranges and needn't reach their ends.
All inputs are finite; a program needn't handle non-finite values.
Results may differ from the reference program's by a relative error of at most 0.0049.
Values may be sent and summed in bfloat16 or wider, within the bound.
No kernel may reach another device: no remote copies, remote signals or barrier semaphores. Data moves between devices by JAX's collectives and lax.ppermute only.
A program may use at most 64 MiB of HBM per device.

```python
import jax
import jax.numpy as jnp
from jax import lax

D = 2048
GROUP = 256
GROUPS = 4
F = 1024
LENGTH = 2048
SEQS = 4


def steps_of(rng, dims, shards, smallest, top_value):
    factor_of = 1.0
    for axis_at, blocks in shards:
        steps = jax.random.uniform(jax.random.fold_in(jax.random.fold_in(rng, 6), axis_at), (blocks,), jnp.float32, smallest / len(shards), top_value / len(shards))
        factor_of = factor_of * jnp.repeat(jnp.exp(steps), dims[axis_at] // blocks).reshape((-1,) + (1,) * (len(dims) - 1 - axis_at))
    return factor_of


def bell_draw(rng, dims, deviation, reach, shards=(), held_as=jnp.bfloat16):
    entries = jax.random.normal(rng, dims, jnp.float32) * deviation
    if len(shards) > 0:
        entries = steps_of(rng, dims, shards, -0.22, 0.18) * entries
    return jnp.clip(entries, min=-reach, max=reach).astype(held_as)


def setup_inputs(seed: int = 0) -> dict:
    key_list = jax.random.split(jax.random.key(seed), 4)
    return {
        "mix_input": bell_draw(key_list[0], (SEQS, LENGTH, F), 1.0, 6.0, ((0, 4), (1, 8))),
        "gate_logits": bell_draw(key_list[1], (SEQS, LENGTH, D), 1.5, 8.0, ((0, 4), (1, 8))),
        "w_proj": bell_draw(key_list[2], (F, D), F ** -0.5, 0.1875, ((0, 4),)),
    }


def reference(mix_input, gate_logits, w_proj):
    def one_sequence(pair_args):
        signal, logits = pair_args
        grouped = signal.astype(jnp.float32).reshape(LENGTH, GROUPS, GROUP)
        spectrum = jnp.real(jnp.fft.fftn(grouped, axes=(0, 2), norm="ortho")).astype(jnp.float32)
        spectrum_bf = spectrum.reshape(LENGTH, GROUPS * GROUP).astype(jnp.bfloat16)
        projected = jnp.dot(spectrum_bf, w_proj, preferred_element_type=jnp.float32)
        return (jax.nn.sigmoid(logits.astype(jnp.float32)) * projected).astype(jnp.bfloat16)

    return lax.map(one_sequence, (mix_input, gate_logits))
```

```python
import functools
import math

import jax
import jax.numpy as jnp
import numpy as np
from jax import lax
from jax.experimental import pallas as pl
from jax.experimental.pallas import tpu as pltpu
from jax.sharding import PartitionSpec as P

GROUP = 256
CHUNKS = 2
MIB = 1 << 20


def split_halves(table):
    head = table.astype(jnp.bfloat16)
    return head, (table - head.astype(np.float64)).astype(jnp.bfloat16)


def feature_table(pairs):
    chunks = GROUP // (2 * pairs)
    out = np.zeros((chunks, 2 * pairs, GROUP))
    m = np.arange(GROUP)
    for t in range(chunks):
        for j in range(pairs):
            c = pairs * t + j
            out[t, j] = np.cos(2 * math.pi * (m * c % GROUP) / GROUP)
            out[t, pairs + j] = -np.sin(2 * math.pi * (m * c % GROUP) / GROUP)
        if t == 0:
            out[0, pairs] = np.where(m % 2 == 0, 1.0, -1.0)
    return out


def position_table(inner, scale):
    angle = 2 * math.pi * (np.outer(np.arange(inner), np.arange(inner)) % inner) / inner
    return np.concatenate([np.cos(angle), np.sin(angle)], axis=1) * scale


def twist_table(rows, inner):
    length = rows * inner
    n2 = np.arange(inner)[:, None]
    res = []
    for core in range(2):
        k1 = 2 * np.arange(rows // 2)[None, :] + core
        angle = 2 * math.pi * (n2 * k1 % length) / length
        res.append(np.concatenate([np.cos(angle), np.sin(angle)], axis=1))
    return np.stack(res).astype(np.float32)


def vmem_call(body, outs, scratch, flops, moved, limit=24):
    return pl.pallas_call(
        body,
        out_shape=outs,
        scratch_shapes=scratch,
        compiler_params=pltpu.CompilerParams(vmem_limit_bytes=limit * MIB),
        cost_estimate=pl.CostEstimate(flops=flops, bytes_accessed=moved, transcendentals=0),
    )


def pick_kernel(rows, chips, q, x_ref, *outs):
    chip = lax.axis_index("row") // 2
    lanes = outs[0].shape[1]
    pairs = lanes // 2
    chips_per_group = GROUP // (CHUNKS * lanes)
    src = lax.broadcasted_iota(jnp.int32, (GROUP, lanes), 0)
    lane = lax.broadcasted_iota(jnp.int32, (GROUP, lanes), 1)
    for zs in range(chips):
        dest = chip ^ zs
        group = dest // chips_per_group
        part = (dest % chips_per_group) * CHUNKS + q
        j = lane - pairs
        mirrored = jnp.where((j == 0) & (part == 0), GROUP // 2, GROUP - pairs * part - j)
        wanted = jnp.where(lane < pairs, pairs * part + lane, mirrored)
        choose = (src == wanted).astype(jnp.bfloat16)
        block = x_ref[:, pl.ds(pl.multiple_of(group * GROUP, GROUP), GROUP)]
        outs[zs][...] = jnp.dot(block, choose, preferred_element_type=jnp.float32).astype(
            jnp.bfloat16
        )


def complex_dft(values):
    n = len(values)
    if n == 1:
        return values
    even, odd = complex_dft(values[0::2]), complex_dft(values[1::2])
    low, high = [], []
    for k in range(n // 2):
        c, s = math.cos(2 * math.pi * k / n), math.sin(2 * math.pi * k / n)
        re, im = odd[k]
        if k == 0:
            tr, ti = re, im
        elif 4 * k == n:
            tr, ti = im, -re
        else:
            tr, ti = re * c + im * s, im * c - re * s
        er, ei = even[k]
        low.append((er + tr, ei + ti))
        high.append((er - tr, ei - ti))
    return low + high


def position_kernel(rows, q, *refs):
    chips = rows // 2
    mine, theirs = refs[:chips], refs[chips]
    table_hi, table_lo, twist = refs[chips + 1 : chips + 4]
    outs = refs[chips + 4 : 2 * chips + 4]
    folded, z_hi, z_lo, spect = refs[2 * chips + 4 :]
    inner, lanes = mine[0].shape
    pairs = lanes // 2
    row = lax.axis_index("row")
    core, chip = row % 2, row // 2
    half = rows // 2

    lane = lax.broadcasted_iota(jnp.int32, (1, lanes), 1)
    chips_per_group = GROUP // (CHUNKS * lanes)
    first = (chip % chips_per_group == 0) if q == 0 else False
    lone_low = (lane == 0) & first
    lone_high = (lane == pairs) & first
    own = jnp.where((lane < pairs) | lone_high, 1.0, -1.0).astype(jnp.float32)
    other = jnp.where(lone_low | lone_high, 0.0, 1.0).astype(jnp.float32)
    cosine = (lane < pairs) | lone_high

    def fold(block):
        value = block.astype(jnp.float32)
        if lanes % 128 == 0:
            turned = pltpu.roll(value, pairs, 1)
        else:
            turned = jnp.concatenate([value[:, pairs:], value[:, :pairs]], axis=1)
        return value * own + turned * other

    for zs in range(chips):
        folded[row ^ (2 * zs)] = fold(mine[zs][...])
        folded[row ^ (2 * zs + 1)] = fold(theirs[zs])

    odd_core = core == 1
    sign = jnp.where(odd_core, -1.0, 1.0).astype(jnp.float32)
    turns = []
    for n in range(half):
        angle = 2 * math.pi * n / rows
        turns.append(
            (
                jnp.where(odd_core, math.cos(angle), 1.0).astype(jnp.float32),
                jnp.where(odd_core, -math.sin(angle), 0.0).astype(jnp.float32),
            )
        )
    tile = min(inner, 32)

    def step(i, carry):
        at = pl.ds(pl.multiple_of(i * tile, tile), tile)
        low_at = pl.ds(pl.multiple_of(inner + i * tile, tile), tile)
        values = []
        for n in range(half):
            v = folded[n, at, :] + sign * folded[n + half, at, :]
            values.append((v * turns[n][0], v * turns[n][1]))
        tw = twist[core, at, :]
        for j, (re, im) in enumerate(complex_dft(values)):
            a = jnp.where(cosine, re, -im)
            b = jnp.where(cosine, im, re)
            c, s = tw[:, j : j + 1], tw[:, half + j : half + j + 1]
            for where, z in ((at, a * c + b * s), (low_at, b * c - a * s)):
                head = z.astype(jnp.bfloat16)
                cols = slice(j * lanes, (j + 1) * lanes)
                z_hi[where, cols] = head
                z_lo[where, cols] = (z - head.astype(jnp.float32)).astype(jnp.bfloat16)
        return carry

    lax.fori_loop(0, inner // tile, step, 0)
    dot = functools.partial(jnp.dot, preferred_element_type=jnp.float32)
    width = min(half * lanes, 256)
    for start in range(0, half * lanes, width):
        cols = slice(start, start + width)
        value = dot(table_hi[...], z_hi[:, cols])
        value += dot(table_hi[...], z_lo[:, cols])
        value += dot(table_lo[...], z_hi[:, cols])
        for j in range(start // lanes, (start + width) // lanes):
            piece = value[:, j * lanes - start : (j + 1) * lanes - start]
            spect[j] = piece
    per = inner // rows
    for zs in range(chips):
        for rel in range(2):
            dest = row ^ (2 * zs + rel)
            for j in range(half):
                outs[zs][rel, j * per : (j + 1) * per, :] = spect[
                    j, pl.ds(pl.multiple_of(dest * per, per), per), :
                ].astype(jnp.bfloat16)


def weight_kernel(x_hi, x_lo, w_ref, own_ref, other_ref):
    core = lax.axis_index("row") % 2
    w = w_ref[...]
    for ref, q in ((own_ref, core), (other_ref, 1 - core)):
        value = jnp.dot(x_hi[q], w, preferred_element_type=jnp.float32)
        value += jnp.dot(x_lo[q], w, preferred_element_type=jnp.float32)
        ref[...] = value.astype(jnp.bfloat16)


def order_rows(rows, count):
    core = lax.axis_index("row") % 2
    half, per = rows // 2, count // rows
    natural = lax.broadcasted_iota(jnp.int32, (count, count), 0)
    received = lax.broadcasted_iota(jnp.int32, (count, count), 1)
    rel, j, k2 = received // (half * per), received // per % half, received % per
    return (natural == rows * k2 + 2 * j + (core ^ rel)).astype(jnp.bfloat16)


def final_kernel(rows, n_col, *refs):
    chips = rows // 2
    mine = [refs[q * (chips + 1) : q * (chips + 1) + chips] for q in range(CHUNKS)]
    theirs = [refs[q * (chips + 1) + chips] for q in range(CHUNKS)]
    at = CHUNKS * (chips + 1)
    w_own = refs[at : at + n_col]
    w_other = refs[at + n_col : at + 2 * n_col]
    gate_ref, out_ref, lhs = refs[at + 2 * n_col :]
    count, lanes = gate_ref.shape[0], mine[0][0].shape[2]
    row, col = lax.axis_index("row"), lax.axis_index("col")
    core, chip = row % 2, row // 2
    order = order_rows(rows, count)
    for q in range(CHUNKS):
        spot = pl.ds(pl.multiple_of((core ^ q) * lanes, lanes), lanes)
        for zs in range(chips):
            got = jnp.concatenate([mine[q][zs][0], theirs[q][zs]], axis=0)
            lhs[zs, :, spot] = jnp.dot(order, got, preferred_element_type=jnp.float32).astype(
                jnp.bfloat16
            )
    width = 256
    for start in range(0, out_ref.shape[1], width):
        cols = slice(start, start + width)
        total = jnp.zeros((count, width), jnp.float32)
        for s in range(n_col):
            rhs = jnp.concatenate([w_own[s][:, cols], w_other[s][:, cols]], axis=0)
            total += jnp.dot(lhs[chip ^ col ^ s], rhs, preferred_element_type=jnp.float32)
        gate = gate_ref[:, cols].astype(jnp.float32)
        out_ref[:, cols] = (jax.nn.sigmoid(gate) * total).astype(jnp.bfloat16)


def swap(value, axis, size, bit):
    return lax.ppermute(value, axis, [(i, i ^ bit) for i in range(size)])


def far_first(chips):
    return sorted(range(1, chips), key=lambda zs: -zs)


def across_chips(pieces, rows):
    chips = rows // 2
    got = [pieces[0]] + [None] * (chips - 1)
    for zs in far_first(chips):
        got[zs] = swap(pieces[zs], "row", rows, 2 * zs)
    return got


def on_device(mix_input, gate_logits, w_proj):
    tokens, gate = mix_input[0], gate_logits[0]
    count, features = tokens.shape
    rows, n_col = lax.axis_size("row"), lax.axis_size("col")
    chips = rows // 2
    lanes = features // (chips * CHUNKS)
    half = rows // 2
    scale = 1.0 / math.sqrt(count * rows * GROUP)
    table_hi, table_lo = split_halves(position_table(count, scale))
    twist = twist_table(rows, count)
    feat_hi, feat_lo = split_halves(feature_table(lanes // 2))
    bf = jnp.bfloat16

    arrived = []
    for q in range(CHUNKS):
        picked = vmem_call(
            functools.partial(pick_kernel, rows, chips, q),
            [jax.ShapeDtypeStruct((count, lanes), bf)] * chips,
            [],
            2 * count * GROUP * lanes * chips,
            3 * count * lanes * chips * 2,
        )(tokens)
        arrived.append(across_chips(picked, rows))

    fast = w_proj.shape[0] == GROUP and CHUNKS * lanes == GROUP and n_col == chips
    width = w_proj.shape[1]
    if fast:
        own, other = vmem_call(
            weight_kernel,
            [jax.ShapeDtypeStruct((lanes, width), bf)] * 2,
            [],
            4 * GROUP * GROUP * width,
            2 * GROUP * width * 2,
        )(feat_hi, feat_lo, w_proj)
        w_own = [own] + [swap(own, "col", n_col, s) for s in range(1, n_col)]

    spectra = []
    for q in range(CHUNKS):
        theirs = swap(jnp.stack(arrived[q]), "row", rows, 1)
        sent = vmem_call(
            functools.partial(position_kernel, rows, q),
            [jax.ShapeDtypeStruct((2, half * (count // rows), lanes), bf)] * chips,
            [
                pltpu.VMEM((rows, count, lanes), jnp.float32),
                pltpu.VMEM((2 * count, half * lanes), bf),
                pltpu.VMEM((2 * count, half * lanes), bf),
                pltpu.VMEM((half, count, lanes), jnp.float32),
            ],
            12 * count * count * half * lanes,
            rows * count * lanes * 4,
        )(*arrived[q], theirs, table_hi, table_lo, twist)
        spectra.append(across_chips(sent, rows))

    if fast:
        w_other = [other] + [swap(w, "row", rows, 1) for w in w_own[1:]]
    operands = []
    for q in range(CHUNKS):
        theirs = swap(jnp.stack([piece[1] for piece in spectra[q]]), "row", rows, 1)
        operands += [*spectra[q], theirs]
    if fast:
        mixed = vmem_call(
            functools.partial(final_kernel, rows, n_col),
            jax.ShapeDtypeStruct((count, width), bf),
            [pltpu.VMEM((chips, count, GROUP), bf)],
            2 * count * features * width,
            2 * features * width,
            limit=32,
        )(*operands, *w_own, *w_other, gate)
        return mixed[None]

    weights = lax.all_gather(w_proj, "col", axis=0, tiled=True).reshape(-1, GROUP, width)
    table = jnp.asarray(feature_table(lanes // 2), jnp.float32)
    turned = jnp.einsum(
        "tlm,gmd->gtld", table, weights.astype(jnp.float32), precision=lax.Precision.HIGHEST
    ).astype(bf)
    turned = turned.reshape(chips, CHUNKS, lanes, width)
    order = order_rows(rows, count)
    chip = lax.axis_index("row") // 2
    total = jnp.zeros((count, width), jnp.float32)
    for q in range(CHUNKS):
        base = q * (chips + 1)
        got = jnp.stack(
            [
                jnp.concatenate([operands[base + zs][0], operands[base + chips][zs]], axis=0)
                for zs in range(chips)
            ]
        )
        got = jnp.einsum("kr,zrl->kzl", order, got, preferred_element_type=jnp.float32).astype(bf)
        weight = turned[chip ^ jnp.arange(chips), q].reshape(chips * lanes, width)
        total += jnp.dot(
            got.reshape(count, chips * lanes), weight, preferred_element_type=jnp.float32
        )
    return (jax.nn.sigmoid(gate.astype(jnp.float32)) * total).astype(bf)[None]


def solution(mesh):
    spec = P("col", "row", None)
    return jax.shard_map(
        on_device, mesh=mesh, in_specs=(spec, spec, P("col", None)), out_specs=spec, check_vma=False
    )
```

```python
import functools
import math

import jax
import jax.numpy as jnp
import numpy as np
from jax import lax
from jax.experimental import pallas as pl
from jax.experimental.pallas import tpu as pltpu
from jax.sharding import PartitionSpec as P


GROUP = 256
CHUNKS = 2
MIB = 1 << 20


def split_halves(table):
    head = table.astype(jnp.bfloat16)
    return head, (table - head.astype(np.float64)).astype(jnp.bfloat16)


def feature_table(pairs):
    chunks = GROUP // (2 * pairs)
    out = np.zeros((chunks, 2 * pairs, GROUP))
    m = np.arange(GROUP)
    for t in range(chunks):
        for j in range(pairs):
            c = pairs * t + j
            out[t, j] = np.cos(2 * math.pi * (m * c % GROUP) / GROUP)
            out[t, pairs + j] = -np.sin(2 * math.pi * (m * c % GROUP) / GROUP)
        if t == 0:
            out[0, pairs] = np.where(m % 2 == 0, 1.0, -1.0)
    return out


def position_table(inner, scale):
    angle = 2 * math.pi * (np.outer(np.arange(inner), np.arange(inner)) % inner) / inner
    return np.concatenate([np.cos(angle), np.sin(angle)], axis=1) * scale


def twist_table(rows, inner):
    length = rows * inner
    n2 = np.arange(inner)[:, None]
    res = []
    for core in range(2):
        k1 = 2 * np.arange(rows // 2)[None, :] + core
        angle = 2 * math.pi * (n2 * k1 % length) / length
        res.append(np.concatenate([np.cos(angle), np.sin(angle)], axis=1))
    return np.stack(res).astype(np.float32)


def vmem_call(body, outs, scratch, flops, moved, limit=24):
    return pl.pallas_call(
        body,
        out_shape=outs,
        scratch_shapes=scratch,
        compiler_params=pltpu.CompilerParams(vmem_limit_bytes=limit * MIB),
        cost_estimate=pl.CostEstimate(flops=flops, bytes_accessed=moved, transcendentals=0),
    )


def pick_kernel(chips, q, x_ref, *outs):
    chip = lax.axis_index("row") // 2
    lanes = outs[0].shape[1]
    pairs = lanes // 2
    chips_per_group = GROUP // (CHUNKS * lanes)
    src = lax.broadcasted_iota(jnp.int32, (GROUP, lanes), 0)
    lane = lax.broadcasted_iota(jnp.int32, (GROUP, lanes), 1)
    for zs in range(chips):
        dest = chip ^ zs
        group = dest // chips_per_group
        part = (dest % chips_per_group) * CHUNKS + q
        j = lane - pairs
        mirrored = jnp.where((j == 0) & (part == 0), GROUP // 2, GROUP - pairs * part - j)
        wanted = jnp.where(lane < pairs, pairs * part + lane, mirrored)
        choose = (src == wanted).astype(jnp.bfloat16)
        block = x_ref[:, pl.ds(pl.multiple_of(group * GROUP, GROUP), GROUP)]
        outs[zs][...] = jnp.dot(block, choose, preferred_element_type=jnp.float32).astype(
            jnp.bfloat16
        )


def complex_dft(values):
    n = len(values)
    if n == 1:
        return values
    even, odd = complex_dft(values[0::2]), complex_dft(values[1::2])
    low, high = [], []
    for k in range(n // 2):
        c, s = math.cos(2 * math.pi * k / n), math.sin(2 * math.pi * k / n)
        re, im = odd[k]
        if k == 0:
            tr, ti = re, im
        elif 4 * k == n:
            tr, ti = im, -re
        else:
            tr, ti = re * c + im * s, im * c - re * s
        er, ei = even[k]
        low.append((er + tr, ei + ti))
        high.append((er - tr, ei - ti))
    return low + high


def position_kernel(rows, q, *refs):
    chips = rows // 2
    mine, theirs = refs[:chips], refs[chips]
    table_hi, table_lo, twist = refs[chips + 1 : chips + 4]
    outs = refs[chips + 4 : 2 * chips + 4]
    folded, z_hi, z_lo, spect = refs[2 * chips + 4 :]
    inner, lanes = mine[0].shape
    pairs = lanes // 2
    row = lax.axis_index("row")
    core, chip = row % 2, row // 2
    half = rows // 2

    lane = lax.broadcasted_iota(jnp.int32, (1, lanes), 1)
    chips_per_group = GROUP // (CHUNKS * lanes)
    first = (chip % chips_per_group == 0) if q == 0 else False
    lone_low = (lane == 0) & first
    lone_high = (lane == pairs) & first
    own = jnp.where((lane < pairs) | lone_high, 1.0, -1.0).astype(jnp.float32)
    other = jnp.where(lone_low | lone_high, 0.0, 1.0).astype(jnp.float32)
    cosine = (lane < pairs) | lone_high

    def fold(block):
        value = block.astype(jnp.float32)
        if lanes % 128 == 0:
            turned = pltpu.roll(value, pairs, 1)
        else:
            turned = jnp.concatenate([value[:, pairs:], value[:, :pairs]], axis=1)
        return value * own + turned * other

    for zs in range(chips):
        folded[row ^ (2 * zs)] = fold(mine[zs][...])
        folded[row ^ (2 * zs + 1)] = fold(theirs[zs])

    odd_core = core == 1
    sign = jnp.where(odd_core, -1.0, 1.0).astype(jnp.float32)
    turns = []
    for n in range(half):
        angle = 2 * math.pi * n / rows
        turns.append(
            (
                jnp.where(odd_core, math.cos(angle), 1.0).astype(jnp.float32),
                jnp.where(odd_core, -math.sin(angle), 0.0).astype(jnp.float32),
            )
        )
    tile = min(inner, 32)

    def step(i, carry):
        at = pl.ds(pl.multiple_of(i * tile, tile), tile)
        low_at = pl.ds(pl.multiple_of(inner + i * tile, tile), tile)
        values = []
        for n in range(half):
            v = folded[n, at, :] + sign * folded[n + half, at, :]
            values.append((v * turns[n][0], v * turns[n][1]))
        tw = twist[core, at, :]
        for j, (re, im) in enumerate(complex_dft(values)):
            a = jnp.where(cosine, re, -im)
            b = jnp.where(cosine, im, re)
            c, s = tw[:, j : j + 1], tw[:, half + j : half + j + 1]
            for where, z in ((at, a * c + b * s), (low_at, b * c - a * s)):
                head = z.astype(jnp.bfloat16)
                cols = slice(j * lanes, (j + 1) * lanes)
                z_hi[where, cols] = head
                z_lo[where, cols] = (z - head.astype(jnp.float32)).astype(jnp.bfloat16)
        return carry

    lax.fori_loop(0, inner // tile, step, 0)
    dot = functools.partial(jnp.dot, preferred_element_type=jnp.float32)
    width = min(half * lanes, 256)
    for start in range(0, half * lanes, width):
        cols = slice(start, start + width)
        value = dot(table_hi[...], z_hi[:, cols])
        value += dot(table_hi[...], z_lo[:, cols])
        value += dot(table_lo[...], z_hi[:, cols])
        for j in range(start // lanes, (start + width) // lanes):
            piece = value[:, j * lanes - start : (j + 1) * lanes - start]
            spect[j] = piece
    per = inner // rows
    for zs in range(chips):
        for rel in range(2):
            dest = row ^ (2 * zs + rel)
            for j in range(half):
                outs[zs][rel, j * per : (j + 1) * per, :] = spect[
                    j, pl.ds(pl.multiple_of(dest * per, per), per), :
                ].astype(jnp.bfloat16)


def order_rows(rows, count):
    core = lax.axis_index("row") % 2
    half, per = rows // 2, count // rows
    natural = lax.broadcasted_iota(jnp.int32, (count, count), 0)
    received = lax.broadcasted_iota(jnp.int32, (count, count), 1)
    rel, j, k2 = received // (half * per), received // per % half, received % per
    return (natural == rows * k2 + 2 * j + (core ^ rel)).astype(jnp.bfloat16)


def give_kernel(*refs):
    out = refs[-1]
    for zs, ref in enumerate(refs[:-1]):
        out[zs] = ref[1]


def channel_part(order, mine, theirs, feat_hi, feat_lo):
    lanes = feat_hi.shape[0]
    got = jnp.concatenate(
        [jnp.concatenate([m[0], theirs[zs]], axis=0) for zs, m in enumerate(mine)], axis=1
    )
    got = jnp.dot(order, got, preferred_element_type=jnp.float32).astype(jnp.bfloat16)
    parts = []
    for zs in range(len(mine)):
        piece = got[:, zs * lanes : (zs + 1) * lanes]
        part = jnp.dot(piece, feat_hi, preferred_element_type=jnp.float32)
        parts.append(part + jnp.dot(piece, feat_lo, preferred_element_type=jnp.float32))
    return parts


def prepare_kernel(rows, *refs):
    chips = rows // 2
    mine, theirs, feat_hi, feat_lo, gate_ref = refs[:chips], *refs[chips : chips + 4]
    spect, opened = refs[chips + 4 :]
    order = order_rows(rows, gate_ref.shape[0])
    for zs, part in enumerate(channel_part(order, mine, theirs, feat_hi[...], feat_lo[...])):
        spect[zs] = part
    for start in range(0, gate_ref.shape[1], GROUP):
        cols = slice(start, start + GROUP)
        opened[:, cols] = jax.nn.sigmoid(gate_ref[:, cols].astype(jnp.float32))


def final_kernel(rows, n_col, *refs):
    chips = rows // 2
    mine, theirs, feat_hi, feat_lo, spect, opened = refs[:chips], *refs[chips : chips + 5]
    at = chips + 5
    w_here = refs[at]
    w_own = refs[at + 1 : at + n_col]
    w_other = refs[at + n_col : at + 2 * n_col - 1]
    out_ref, lhs, result, sems = refs[at + 2 * n_col - 1 :]
    count, width = opened.shape
    half = GROUP // 2
    row, col = lax.axis_index("row"), lax.axis_index("col")
    core, chip = row % 2, row // 2
    order = order_rows(rows, count)
    for zs, part in enumerate(channel_part(order, mine, theirs, feat_hi[...], feat_lo[...])):
        whole = (part + spect[zs]).astype(jnp.bfloat16)
        for h in range(2):
            spot = pl.ds(pl.multiple_of((core ^ h) * half, half), half)
            lhs[zs, :, spot] = whole[:, h * half : (h + 1) * half]
    copies = []
    for t in range(width // GROUP):
        cols = slice(t * GROUP, (t + 1) * GROUP)
        total = jnp.zeros((count, GROUP), jnp.float32)
        for s in range(n_col):
            if s == 0:
                own = w_here[pl.ds(pl.multiple_of(core * half, half), half), cols]
                other = w_here[pl.ds(pl.multiple_of((1 - core) * half, half), half), cols]
            else:
                own, other = w_own[s - 1][:, cols], w_other[s - 1][:, cols]
            rhs = jnp.concatenate([own, other], axis=0)
            total += jnp.dot(lhs[chip ^ col ^ s], rhs, preferred_element_type=jnp.float32)
        result[:, cols] = (opened[:, cols] * total).astype(jnp.bfloat16)
        copies.append(pltpu.make_async_copy(result.at[:, cols], out_ref.at[:, cols], sems.at[t]))
        copies[-1].start()
    for copy in copies:
        copy.wait()


def swap(value, axis, size, bit):
    return lax.ppermute(value, axis, [(i, i ^ bit) for i in range(size)])


def send_order(chips):
    return sorted(range(1, chips), key=lambda zs: (zs < 2, zs))


def across_chips(pieces, rows):
    chips = rows // 2
    got = [pieces[0]] + [None] * (chips - 1)
    for zs in send_order(chips):
        got[zs] = swap(pieces[zs], "row", rows, 2 * zs)
    return got


def on_device(mix_input, gate_logits, w_proj):
    return program(mix_input[0], gate_logits[0], w_proj)[None]


def program(tokens, gate, w_proj):
    count, features = tokens.shape
    rows, n_col = lax.axis_size("row"), lax.axis_size("col")
    chips = rows // 2
    lanes = features // (chips * CHUNKS)
    half = rows // 2
    width = w_proj.shape[1]
    scale = 1.0 / math.sqrt(count * rows * GROUP)
    table_hi, table_lo = split_halves(position_table(count, scale))
    twist = twist_table(rows, count)
    features_of = feature_table(lanes // 2)
    feat_hi, feat_lo = split_halves(features_of)
    bf = jnp.bfloat16
    fast = w_proj.shape[0] == GROUP and CHUNKS * lanes == GROUP and n_col == chips

    if fast:
        core = lax.axis_index("row") % 2
        mine = lax.dynamic_slice_in_dim(w_proj, core * (GROUP // 2), GROUP // 2, 0)
        w_own = []
        for s in range(1, n_col):
            w_own.append(swap(mine, "col", n_col, s))

    arrived = []
    for q in range(CHUNKS):
        picked = vmem_call(
            functools.partial(pick_kernel, chips, q),
            [jax.ShapeDtypeStruct((count, lanes), bf)] * chips,
            [],
            2 * count * GROUP * lanes * chips,
            3 * count * lanes * chips * 2,
        )(tokens)
        arrived.append(across_chips(picked, rows))

    spectra = []
    for q in range(CHUNKS):
        theirs = swap(jnp.stack(arrived[q]), "row", rows, 1)
        sent = vmem_call(
            functools.partial(position_kernel, rows, q),
            [jax.ShapeDtypeStruct((2, half * (count // rows), lanes), bf)] * chips,
            [
                pltpu.VMEM((rows, count, lanes), jnp.float32),
                pltpu.VMEM((2 * count, half * lanes), bf),
                pltpu.VMEM((2 * count, half * lanes), bf),
                pltpu.VMEM((half, count, lanes), jnp.float32),
            ],
            12 * count * count * half * lanes,
            rows * count * lanes * 4,
        )(*arrived[q], theirs, table_hi, table_lo, twist)
        spectra.append(across_chips(sent, rows))

    if fast:
        w_other = []
        for s in range(1, n_col):
            w_other.append(swap(w_own[s - 1], "row", rows, 1))
    operands = []
    for q in range(CHUNKS):
        give = vmem_call(
            give_kernel,
            jax.ShapeDtypeStruct((chips, half * (count // rows), lanes), bf),
            [],
            count * lanes * chips,
            2 * count * lanes * chips,
        )(*spectra[q])
        theirs = swap(give, "row", rows, 1)
        operands.append([*spectra[q], theirs])
    if fast:
        spect, opened = vmem_call(
            functools.partial(prepare_kernel, rows),
            [
                jax.ShapeDtypeStruct((chips, count, GROUP), jnp.float32),
                jax.ShapeDtypeStruct((count, width), jnp.float32),
            ],
            [],
            2 * count * features * GROUP,
            6 * count * width,
        )(*operands[0], feat_hi[0], feat_lo[0], gate)
        return pl.pallas_call(
            functools.partial(final_kernel, rows, n_col),
            out_shape=jax.ShapeDtypeStruct((count, width), bf),
            in_specs=[pl.BlockSpec(memory_space=pltpu.VMEM)] * (chips + 5 + 2 * n_col - 1),
            out_specs=pl.BlockSpec(memory_space=pl.ANY),
            scratch_shapes=[
                pltpu.VMEM((chips, count, GROUP), bf),
                pltpu.VMEM((count, width), bf),
                pltpu.SemaphoreType.DMA((width // GROUP,)),
            ],
            compiler_params=pltpu.CompilerParams(vmem_limit_bytes=32 * MIB),
            cost_estimate=pl.CostEstimate(
                flops=2 * count * features * width,
                bytes_accessed=2 * features * width,
                transcendentals=0,
            ),
        )(*operands[1], feat_hi[1], feat_lo[1], spect, opened, w_proj, *w_own, *w_other)

    weights = lax.all_gather(w_proj, "col", axis=0, tiled=True).reshape(-1, GROUP, width)
    order = order_rows(rows, count)
    chip = lax.axis_index("row") // 2
    table = jnp.asarray(features_of, jnp.float32).reshape(-1, CHUNKS, lanes, GROUP)
    per_group = table.shape[0]
    spectrum = jnp.zeros((count, weights.shape[0], GROUP), jnp.float32)
    here = chip ^ jnp.arange(chips)
    for q in range(CHUNKS):
        got = jnp.stack(
            [
                jnp.concatenate([operands[q][zs][0], operands[q][chips][zs]], axis=0)
                for zs in range(chips)
            ]
        )[here]
        got = jnp.einsum("kr,zrl->kzl", order, got, preferred_element_type=jnp.float32)
        spectrum += jnp.einsum(
            "kgtl,tlm->kgm",
            got.reshape(count, -1, per_group, lanes),
            table[:, q],
            precision=lax.Precision.HIGHEST,
        )
    total = jnp.einsum(
        "kgm,gmd->kd", spectrum.astype(bf), weights, preferred_element_type=jnp.float32
    )
    return (jax.nn.sigmoid(gate.astype(jnp.float32)) * total).astype(bf)


def solution(mesh):
    spec = P("col", "row", None)
    return jax.shard_map(
        on_device, mesh=mesh, in_specs=(spec, spec, P("col", None)), out_specs=spec, check_vma=False
    )
```

```python
import functools
import math

import jax
import jax.numpy as jnp
import numpy as np
from jax import lax
from jax.experimental import pallas as pl
from jax.experimental.pallas import tpu as pltpu
from jax.sharding import PartitionSpec as P


GROUP = 256
CHUNKS = 2
MIB = 1 << 20


def split_halves(table):
    head = table.astype(jnp.bfloat16)
    return head, (table - head.astype(np.float64)).astype(jnp.bfloat16)


def feature_table(pairs):
    chunks = GROUP // (2 * pairs)
    out = np.zeros((chunks, 2 * pairs, GROUP))
    m = np.arange(GROUP)
    for t in range(chunks):
        for j in range(pairs):
            c = pairs * t + j
            out[t, j] = np.cos(2 * math.pi * (m * c % GROUP) / GROUP)
            out[t, pairs + j] = -np.sin(2 * math.pi * (m * c % GROUP) / GROUP)
        if t == 0:
            out[0, pairs] = np.where(m % 2 == 0, 1.0, -1.0)
    return out


def position_table(inner, scale):
    angle = 2 * math.pi * (np.outer(np.arange(inner), np.arange(inner)) % inner) / inner
    return np.concatenate([np.cos(angle), np.sin(angle)], axis=1) * scale


def twist_table(rows, inner):
    length = rows * inner
    n2 = np.arange(inner)[:, None]
    res = []
    for core in range(2):
        k1 = 2 * np.arange(rows // 2)[None, :] + core
        angle = 2 * math.pi * (n2 * k1 % length) / length
        res.append(np.concatenate([np.cos(angle), np.sin(angle)], axis=1))
    return np.stack(res).astype(np.float32)


def vmem_call(body, outs, scratch, flops, moved, limit=24):
    return pl.pallas_call(
        body,
        out_shape=outs,
        scratch_shapes=scratch,
        compiler_params=pltpu.CompilerParams(vmem_limit_bytes=limit * MIB),
        cost_estimate=pl.CostEstimate(flops=flops, bytes_accessed=moved, transcendentals=0),
    )


def pick_kernel(chips, q, x_ref, *outs):
    chip = lax.axis_index("row") // 2
    lanes = outs[0].shape[1]
    pairs = lanes // 2
    chips_per_group = GROUP // (CHUNKS * lanes)
    src = lax.broadcasted_iota(jnp.int32, (GROUP, lanes), 0)
    lane = lax.broadcasted_iota(jnp.int32, (GROUP, lanes), 1)
    for zs in range(chips):
        dest = chip ^ zs
        group = dest // chips_per_group
        part = (dest % chips_per_group) * CHUNKS + q
        j = lane - pairs
        mirrored = jnp.where((j == 0) & (part == 0), GROUP // 2, GROUP - pairs * part - j)
        wanted = jnp.where(lane < pairs, pairs * part + lane, mirrored)
        choose = (src == wanted).astype(jnp.bfloat16)
        block = x_ref[:, pl.ds(pl.multiple_of(group * GROUP, GROUP), GROUP)]
        outs[zs][...] = jnp.dot(block, choose, preferred_element_type=jnp.float32).astype(
            jnp.bfloat16
        )


def complex_dft(values):
    n = len(values)
    if n == 1:
        return values
    even, odd = complex_dft(values[0::2]), complex_dft(values[1::2])
    low, high = [], []
    for k in range(n // 2):
        c, s = math.cos(2 * math.pi * k / n), math.sin(2 * math.pi * k / n)
        re, im = odd[k]
        if k == 0:
            tr, ti = re, im
        elif 4 * k == n:
            tr, ti = im, -re
        else:
            tr, ti = re * c + im * s, im * c - re * s
        er, ei = even[k]
        low.append((er + tr, ei + ti))
        high.append((er - tr, ei - ti))
    return low + high


def position_kernel(rows, q, *refs):
    chips = rows // 2
    mine, theirs = refs[:chips], refs[chips]
    table_hi, table_lo, twist = refs[chips + 1 : chips + 4]
    outs = refs[chips + 4 : 2 * chips + 4]
    folded, z_hi, z_lo, spect = refs[2 * chips + 4 :]
    inner, lanes = mine[0].shape
    pairs = lanes // 2
    row = lax.axis_index("row")
    core, chip = row % 2, row // 2
    half = rows // 2

    lane = lax.broadcasted_iota(jnp.int32, (1, lanes), 1)
    chips_per_group = GROUP // (CHUNKS * lanes)
    first = (chip % chips_per_group == 0) if q == 0 else False
    lone_low = (lane == 0) & first
    lone_high = (lane == pairs) & first
    own = jnp.where((lane < pairs) | lone_high, 1.0, -1.0).astype(jnp.float32)
    other = jnp.where(lone_low | lone_high, 0.0, 1.0).astype(jnp.float32)
    cosine = (lane < pairs) | lone_high

    def fold(block):
        value = block.astype(jnp.float32)
        if lanes % 128 == 0:
            turned = pltpu.roll(value, pairs, 1)
        else:
            turned = jnp.concatenate([value[:, pairs:], value[:, :pairs]], axis=1)
        return value * own + turned * other

    for zs in range(chips):
        folded[row ^ (2 * zs)] = fold(mine[zs][...])
        folded[row ^ (2 * zs + 1)] = fold(theirs[zs])

    odd_core = core == 1
    sign = jnp.where(odd_core, -1.0, 1.0).astype(jnp.float32)
    turns = []
    for n in range(half):
        angle = 2 * math.pi * n / rows
        turns.append(
            (
                jnp.where(odd_core, math.cos(angle), 1.0).astype(jnp.float32),
                jnp.where(odd_core, -math.sin(angle), 0.0).astype(jnp.float32),
            )
        )
    tile = min(inner, 32)

    def step(i, carry):
        at = pl.ds(pl.multiple_of(i * tile, tile), tile)
        low_at = pl.ds(pl.multiple_of(inner + i * tile, tile), tile)
        values = []
        for n in range(half):
            v = folded[n, at, :] + sign * folded[n + half, at, :]
            values.append((v * turns[n][0], v * turns[n][1]))
        tw = twist[core, at, :]
        for j, (re, im) in enumerate(complex_dft(values)):
            a = jnp.where(cosine, re, -im)
            b = jnp.where(cosine, im, re)
            c, s = tw[:, j : j + 1], tw[:, half + j : half + j + 1]
            for where, z in ((at, a * c + b * s), (low_at, b * c - a * s)):
                head = z.astype(jnp.bfloat16)
                cols = slice(j * lanes, (j + 1) * lanes)
                z_hi[where, cols] = head
                z_lo[where, cols] = (z - head.astype(jnp.float32)).astype(jnp.bfloat16)
        return carry

    lax.fori_loop(0, inner // tile, step, 0)
    dot = functools.partial(jnp.dot, preferred_element_type=jnp.float32)
    width = min(half * lanes, 256)
    for start in range(0, half * lanes, width):
        cols = slice(start, start + width)
        value = dot(table_hi[...], z_hi[:, cols])
        value += dot(table_hi[...], z_lo[:, cols])
        value += dot(table_lo[...], z_hi[:, cols])
        for j in range(start // lanes, (start + width) // lanes):
            piece = value[:, j * lanes - start : (j + 1) * lanes - start]
            spect[j] = piece
    per = inner // rows
    for zs in range(chips):
        for rel in range(2):
            dest = row ^ (2 * zs + rel)
            for j in range(half):
                outs[zs][rel, j * per : (j + 1) * per, :] = spect[
                    j, pl.ds(pl.multiple_of(dest * per, per), per), :
                ].astype(jnp.bfloat16)


def order_rows(rows, count):
    core = lax.axis_index("row") % 2
    half, per = rows // 2, count // rows
    natural = lax.broadcasted_iota(jnp.int32, (count, count), 0)
    received = lax.broadcasted_iota(jnp.int32, (count, count), 1)
    rel, j, k2 = received // (half * per), received // per % half, received % per
    return (natural == rows * k2 + 2 * j + (core ^ rel)).astype(jnp.bfloat16)


def give_kernel(*refs):
    out = refs[-1]
    for zs, ref in enumerate(refs[:-1]):
        out[zs] = ref[1]


def channel_part(order, mine, theirs, feat_hi, feat_lo):
    lanes = feat_hi.shape[0]
    got = jnp.concatenate(
        [jnp.concatenate([m[0], theirs[zs]], axis=0) for zs, m in enumerate(mine)], axis=1
    )
    got = jnp.dot(order, got, preferred_element_type=jnp.float32).astype(jnp.bfloat16)
    parts = []
    for zs in range(len(mine)):
        piece = got[:, zs * lanes : (zs + 1) * lanes]
        part = jnp.dot(piece, feat_hi, preferred_element_type=jnp.float32)
        parts.append(part + jnp.dot(piece, feat_lo, preferred_element_type=jnp.float32))
    return parts


def prepare_kernel(rows, *refs):
    chips = rows // 2
    mine, theirs, feat_hi, feat_lo, gate_ref = refs[:chips], *refs[chips : chips + 4]
    spect, opened = refs[chips + 4 :]
    order = order_rows(rows, gate_ref.shape[0])
    for zs, part in enumerate(channel_part(order, mine, theirs, feat_hi[...], feat_lo[...])):
        spect[zs] = part
    for start in range(0, gate_ref.shape[1], GROUP):
        cols = slice(start, start + GROUP)
        opened[:, cols] = jax.nn.sigmoid(gate_ref[:, cols].astype(jnp.float32))


def cut_kernel(w_ref, out_ref):
    half = GROUP // 2
    core = lax.axis_index("row") % 2
    out_ref[...] = w_ref[pl.ds(pl.multiple_of(core * half, half), half), :]


def relay_kernel(first, second, to_first, to_second):
    rows = to_first.shape[0]
    to_first[...] = second[:rows, :]
    to_second[...] = first[rows:, :]


def final_kernel(rows, *refs):
    chips = rows // 2
    mine, theirs, feat_hi, feat_lo, spect, opened = refs[:chips], *refs[chips : chips + 5]
    w_here, *w_far, out_ref, lhs, result, sems = refs[chips + 5 :]
    count, width = opened.shape
    half = GROUP // 2
    row, col = lax.axis_index("row"), lax.axis_index("col")
    core, chip = row % 2, row // 2
    order = order_rows(rows, count)
    for zs, part in enumerate(channel_part(order, mine, theirs, feat_hi[...], feat_lo[...])):
        whole = (part + spect[zs]).astype(jnp.bfloat16)
        for h in range(2):
            spot = pl.ds(pl.multiple_of((core ^ h) * half, half), half)
            lhs[zs, :, spot] = whole[:, h * half : (h + 1) * half]
    first, second, low, high = (w_far[i::4] for i in range(4))
    copies = []
    for t in range(width // GROUP):
        cols = slice(t * GROUP, (t + 1) * GROUP)
        total = jnp.zeros((count, GROUP), jnp.float32)
        for s in range(4):
            if s == 0:
                parts = [
                    w_here[pl.ds(pl.multiple_of(h * half, half), half), cols]
                    for h in (core, 1 - core)
                ]
            elif s < 3:
                parts = [ref[:, cols] for ref in (first, second)[s - 1]]
            else:
                parts = [ref[:, cols] for pair in zip(low, high) for ref in pair]
            rhs = jnp.concatenate(parts, axis=0)
            total += jnp.dot(lhs[chip ^ col ^ s], rhs, preferred_element_type=jnp.float32)
        result[:, cols] = (opened[:, cols] * total).astype(jnp.bfloat16)
        copies.append(pltpu.make_async_copy(result.at[:, cols], out_ref.at[:, cols], sems.at[t]))
        copies[-1].start()
    for copy in copies:
        copy.wait()


def swap(value, axis, size, bit):
    return lax.ppermute(value, axis, [(i, i ^ bit) for i in range(size)])


def send_order(chips):
    return sorted(range(1, chips), key=lambda zs: (zs < 2, zs))


def across_chips(pieces, rows):
    chips = rows // 2
    got = [pieces[0]] + [None] * (chips - 1)
    for zs in send_order(chips):
        got[zs] = swap(pieces[zs], "row", rows, 2 * zs)
    return got


def on_device(mix_input, gate_logits, w_proj):
    return program(mix_input[0], gate_logits[0], w_proj)[None]


def program(tokens, gate, w_proj):
    count, features = tokens.shape
    rows, n_col = lax.axis_size("row"), lax.axis_size("col")
    chips = rows // 2
    lanes = features // (chips * CHUNKS)
    half = rows // 2
    width = w_proj.shape[1]
    scale = 1.0 / math.sqrt(count * rows * GROUP)
    table_hi, table_lo = split_halves(position_table(count, scale))
    twist = twist_table(rows, count)
    features_of = feature_table(lanes // 2)
    feat_hi, feat_lo = split_halves(features_of)
    bf = jnp.bfloat16
    fast = w_proj.shape[0] == GROUP and CHUNKS * lanes == GROUP and n_col == chips == 4

    arrived = []
    for q in range(CHUNKS):
        picked = vmem_call(
            functools.partial(pick_kernel, chips, q),
            [jax.ShapeDtypeStruct((count, lanes), bf)] * chips,
            [],
            2 * count * GROUP * lanes * chips,
            3 * count * lanes * chips * 2,
        )(tokens)
        arrived.append(across_chips(picked, rows))

    if fast:
        w_own = []
        piece = jax.ShapeDtypeStruct((GROUP // 2, width), bf)
        part = jax.ShapeDtypeStruct((GROUP // 4, width), bf)
        mine = vmem_call(cut_kernel, piece, [], GROUP * width, 2 * GROUP * width)(w_proj)
        for s in (1, 2):
            w_own.append(swap(mine, "col", n_col, s))
        passed = vmem_call(relay_kernel, [part] * 2, [], GROUP * width, 2 * GROUP * width)(*w_own)
        for s in (1, 2):
            w_own.append(swap(passed[s - 1], "col", n_col, s))

    spectra = []
    for q in range(CHUNKS):
        theirs = swap(jnp.stack(arrived[q]), "row", rows, 1)
        sent = vmem_call(
            functools.partial(position_kernel, rows, q),
            [jax.ShapeDtypeStruct((2, half * (count // rows), lanes), bf)] * chips,
            [
                pltpu.VMEM((rows, count, lanes), jnp.float32),
                pltpu.VMEM((2 * count, half * lanes), bf),
                pltpu.VMEM((2 * count, half * lanes), bf),
                pltpu.VMEM((half, count, lanes), jnp.float32),
            ],
            12 * count * count * half * lanes,
            rows * count * lanes * 4,
        )(*arrived[q], theirs, table_hi, table_lo, twist)
        spectra.append(across_chips(sent, rows))

    if fast:
        w_other = []
        for own in w_own:
            w_other.append(swap(own, "row", rows, 1))
    operands = []
    for q in range(CHUNKS):
        give = vmem_call(
            give_kernel,
            jax.ShapeDtypeStruct((chips, half * (count // rows), lanes), bf),
            [],
            count * lanes * chips,
            2 * count * lanes * chips,
        )(*spectra[q])
        theirs = swap(give, "row", rows, 1)
        operands.append([*spectra[q], theirs])
    if fast:
        spect, opened = vmem_call(
            functools.partial(prepare_kernel, rows),
            [
                jax.ShapeDtypeStruct((chips, count, GROUP), jnp.float32),
                jax.ShapeDtypeStruct((count, width), jnp.float32),
            ],
            [],
            2 * count * features * GROUP,
            6 * count * width,
        )(*operands[0], feat_hi[0], feat_lo[0], gate)
        return pl.pallas_call(
            functools.partial(final_kernel, rows),
            out_shape=jax.ShapeDtypeStruct((count, width), bf),
            in_specs=[pl.BlockSpec(memory_space=pltpu.VMEM)] * (chips + 14),
            out_specs=pl.BlockSpec(memory_space=pl.ANY),
            scratch_shapes=[
                pltpu.VMEM((chips, count, GROUP), bf),
                pltpu.VMEM((count, width), bf),
                pltpu.SemaphoreType.DMA((width // GROUP,)),
            ],
            compiler_params=pltpu.CompilerParams(vmem_limit_bytes=32 * MIB),
            cost_estimate=pl.CostEstimate(
                flops=2 * count * features * width,
                bytes_accessed=2 * features * width,
                transcendentals=0,
            ),
        )(*operands[1], feat_hi[1], feat_lo[1], spect, opened, w_proj, *w_own, *w_other)

    weights = lax.all_gather(w_proj, "col", axis=0, tiled=True).reshape(-1, GROUP, width)
    order = order_rows(rows, count)
    chip = lax.axis_index("row") // 2
    table = jnp.asarray(features_of, jnp.float32).reshape(-1, CHUNKS, lanes, GROUP)
    per_group = table.shape[0]
    spectrum = jnp.zeros((count, weights.shape[0], GROUP), jnp.float32)
    here = chip ^ jnp.arange(chips)
    for q in range(CHUNKS):
        got = jnp.stack(
            [
                jnp.concatenate([operands[q][zs][0], operands[q][chips][zs]], axis=0)
                for zs in range(chips)
            ]
        )[here]
        got = jnp.einsum("kr,zrl->kzl", order, got, preferred_element_type=jnp.float32)
        spectrum += jnp.einsum(
            "kgtl,tlm->kgm",
            got.reshape(count, -1, per_group, lanes),
            table[:, q],
            precision=lax.Precision.HIGHEST,
        )
    total = jnp.einsum(
        "kgm,gmd->kd", spectrum.astype(bf), weights, preferred_element_type=jnp.float32
    )
    return (jax.nn.sigmoid(gate.astype(jnp.float32)) * total).astype(bf)


def solution(mesh):
    spec = P("col", "row", None)
    return jax.shard_map(
        on_device, mesh=mesh, in_specs=(spec, spec, P("col", None)), out_specs=spec, check_vma=False
    )
```

```python
import functools
import math

import jax
import jax.numpy as jnp
import numpy as np
from jax import lax
from jax.experimental import pallas as pl
from jax.experimental.pallas import tpu as pltpu
from jax.sharding import PartitionSpec as P


GROUP = 256
CHUNKS = 2
MIB = 1 << 20


def split_halves(table):
    head = table.astype(jnp.bfloat16)
    return head, (table - head.astype(np.float64)).astype(jnp.bfloat16)


def feature_table(pairs):
    chunks = GROUP // (2 * pairs)
    out = np.zeros((chunks, 2 * pairs, GROUP))
    m = np.arange(GROUP)
    for t in range(chunks):
        for j in range(pairs):
            c = pairs * t + j
            out[t, j] = np.cos(2 * math.pi * (m * c % GROUP) / GROUP)
            out[t, pairs + j] = -np.sin(2 * math.pi * (m * c % GROUP) / GROUP)
        if t == 0:
            out[0, pairs] = np.where(m % 2 == 0, 1.0, -1.0)
    return out


def position_table(inner, scale):
    angle = 2 * math.pi * (np.outer(np.arange(inner), np.arange(inner)) % inner) / inner
    return np.concatenate([np.cos(angle), np.sin(angle)], axis=1) * scale


def twist_table(rows, inner):
    length = rows * inner
    n2 = np.arange(inner)[:, None]
    res = []
    for core in range(2):
        k1 = 2 * np.arange(rows // 2)[None, :] + core
        angle = 2 * math.pi * (n2 * k1 % length) / length
        res.append(np.concatenate([np.cos(angle), np.sin(angle)], axis=1))
    return np.stack(res).astype(np.float32)


def vmem_call(body, outs, scratch, flops, moved, limit=24):
    return pl.pallas_call(
        body,
        out_shape=outs,
        scratch_shapes=scratch,
        compiler_params=pltpu.CompilerParams(vmem_limit_bytes=limit * MIB),
        cost_estimate=pl.CostEstimate(flops=flops, bytes_accessed=moved, transcendentals=0),
    )


def pick_kernel(chips, fast, *refs):
    x_ref, w_ref = refs[:2]
    outs = refs[2 : 2 + chips]
    halves = refs[2 + chips : -3]
    tokens, x_sems, w_sems = refs[-3:]
    row = lax.axis_index("row")
    core, chip = row % 2, row // 2
    lanes = outs[0].shape[2]
    pairs = lanes // 2
    chips_per_group = GROUP // (CHUNKS * lanes)
    loads = []
    for zs in range(chips):
        group = (chip ^ zs) // chips_per_group
        columns = pl.ds(pl.multiple_of(group * GROUP, GROUP), GROUP)
        loads.append(pltpu.make_async_copy(x_ref.at[:, columns], tokens.at[zs], x_sems.at[zs]))
    order = [*send_order(chips), 0]
    for zs in order:
        loads[zs].start()
    fetches = []
    if fast:
        half = GROUP // 2
        for i, h in enumerate((core, 1 - core)):
            part = w_ref.at[pl.ds(pl.multiple_of(h * half, half), half), :]
            fetches.append(pltpu.make_async_copy(part, halves[i], w_sems.at[i]))
            fetches[-1].start()
    src = lax.broadcasted_iota(jnp.int32, (GROUP, CHUNKS * lanes), 0)
    column = lax.broadcasted_iota(jnp.int32, (GROUP, CHUNKS * lanes), 1)
    lane, j = column % lanes, column % lanes - pairs
    for zs in order:
        part = ((chip ^ zs) % chips_per_group) * CHUNKS + column // lanes
        mirrored = jnp.where((j == 0) & (part == 0), GROUP // 2, GROUP - pairs * part - j)
        wanted = jnp.where(lane < pairs, pairs * part + lane, mirrored)
        choose = (src == wanted).astype(jnp.bfloat16)
        loads[zs].wait()
        got = jnp.dot(tokens[zs], choose, preferred_element_type=jnp.float32).astype(jnp.bfloat16)
        for q in range(CHUNKS):
            outs[zs][q] = got[:, q * lanes : (q + 1) * lanes]
    for fetch in fetches:
        fetch.wait()


def stack_kernel(*refs):
    pieces, outs = refs[:-CHUNKS], refs[-CHUNKS:]
    for q, out in enumerate(outs):
        for zs, piece in enumerate(pieces):
            out[zs] = piece[q]


def complex_dft(values):
    n = len(values)
    if n == 1:
        return values
    even, odd = complex_dft(values[0::2]), complex_dft(values[1::2])
    low, high = [], []
    for k in range(n // 2):
        c, s = math.cos(2 * math.pi * k / n), math.sin(2 * math.pi * k / n)
        re, im = odd[k]
        if k == 0:
            tr, ti = re, im
        elif 4 * k == n:
            tr, ti = im, -re
        else:
            tr, ti = re * c + im * s, im * c - re * s
        er, ei = even[k]
        low.append((er + tr, ei + ti))
        high.append((er - tr, ei - ti))
    return low + high


def position_kernel(rows, q, *refs):
    chips = rows // 2
    mine, theirs = refs[:chips], refs[chips]
    table_hi, table_lo, twist = refs[chips + 1 : chips + 4]
    *outs, folded, z_hi, z_lo, spect = refs[chips + 4 :]
    inner, lanes = mine[0].shape[1:]
    pairs = lanes // 2
    row = lax.axis_index("row")
    core, chip = row % 2, row // 2
    half = rows // 2

    lane = lax.broadcasted_iota(jnp.int32, (1, lanes), 1)
    chips_per_group = GROUP // (CHUNKS * lanes)
    first = (chip % chips_per_group == 0) if q == 0 else False
    lone_low = (lane == 0) & first
    lone_high = (lane == pairs) & first
    own = jnp.where((lane < pairs) | lone_high, 1.0, -1.0).astype(jnp.float32)
    other = jnp.where(lone_low | lone_high, 0.0, 1.0).astype(jnp.float32)
    cosine = (lane < pairs) | lone_high

    def fold(block):
        value = block.astype(jnp.float32)
        if lanes % 128 == 0:
            turned = pltpu.roll(value, pairs, 1)
        else:
            turned = jnp.concatenate([value[:, pairs:], value[:, :pairs]], axis=1)
        return value * own + turned * other

    for zs in range(chips):
        folded[row ^ (2 * zs)] = fold(mine[zs][q])
        folded[row ^ (2 * zs + 1)] = fold(theirs[zs])

    odd_core = core == 1
    sign = jnp.where(odd_core, -1.0, 1.0).astype(jnp.float32)
    turns = []
    for n in range(half):
        angle = 2 * math.pi * n / rows
        turns.append(
            (
                jnp.where(odd_core, math.cos(angle), 1.0).astype(jnp.float32),
                jnp.where(odd_core, -math.sin(angle), 0.0).astype(jnp.float32),
            )
        )
    tile = min(inner, 32)

    def step(i, carry):
        at = pl.ds(pl.multiple_of(i * tile, tile), tile)
        low_at = pl.ds(pl.multiple_of(inner + i * tile, tile), tile)
        values = []
        for n in range(half):
            v = folded[n, at, :] + sign * folded[n + half, at, :]
            values.append((v * turns[n][0], v * turns[n][1]))
        tw = twist[core, at, :]
        for j, (re, im) in enumerate(complex_dft(values)):
            a = jnp.where(cosine, re, -im)
            b = jnp.where(cosine, im, re)
            c, s = tw[:, j : j + 1], tw[:, half + j : half + j + 1]
            for where, z in ((at, a * c + b * s), (low_at, b * c - a * s)):
                head = z.astype(jnp.bfloat16)
                cols = slice(j * lanes, (j + 1) * lanes)
                z_hi[where, cols] = head
                z_lo[where, cols] = (z - head.astype(jnp.float32)).astype(jnp.bfloat16)
        return carry

    lax.fori_loop(0, inner // tile, step, 0)
    dot = functools.partial(jnp.dot, preferred_element_type=jnp.float32)
    width = min(half * lanes, 256)
    for start in range(0, half * lanes, width):
        cols = slice(start, start + width)
        value = dot(table_hi[...], z_hi[:, cols])
        value += dot(table_hi[...], z_lo[:, cols])
        value += dot(table_lo[...], z_hi[:, cols])
        for j in range(start // lanes, (start + width) // lanes):
            piece = value[:, j * lanes - start : (j + 1) * lanes - start]
            spect[j] = piece
    per = inner // rows
    for zs in range(chips):
        for rel in range(2):
            dest = row ^ (2 * zs + rel)
            for j in range(half):
                piece = spect[j, pl.ds(pl.multiple_of(dest * per, per), per), :]
                lines = slice(j * per, (j + 1) * per)
                if q == 0:
                    outs[zs][rel, lines, :] = piece.astype(jnp.bfloat16)
                else:
                    outs[rel][zs, lines, :] = piece.astype(jnp.bfloat16)


def order_rows(rows, count):
    core = lax.axis_index("row") % 2
    half, per = rows // 2, count // rows
    natural = lax.broadcasted_iota(jnp.int32, (count, count), 0)
    received = lax.broadcasted_iota(jnp.int32, (count, count), 1)
    rel, j, k2 = received // (half * per), received // per % half, received % per
    return (natural == rows * k2 + 2 * j + (core ^ rel)).astype(jnp.bfloat16)


def give_kernel(*refs):
    out = refs[-1]
    for zs, ref in enumerate(refs[:-1]):
        out[zs] = ref[1]


def join_kernel(keep, got, *outs):
    for zs, out in enumerate(outs):
        out[0] = keep[zs]
        out[1] = got[zs]


def channel_part(order, pieces, feat_hi, feat_lo):
    lanes = feat_hi.shape[0]
    got = jnp.concatenate([jnp.concatenate(piece, axis=0) for piece in pieces], axis=1)
    got = jnp.dot(order, got, preferred_element_type=jnp.float32).astype(jnp.bfloat16)
    parts = []
    for zs in range(len(pieces)):
        piece = got[:, zs * lanes : (zs + 1) * lanes]
        part = jnp.dot(piece, feat_hi, preferred_element_type=jnp.float32)
        parts.append(part + jnp.dot(piece, feat_lo, preferred_element_type=jnp.float32))
    return parts


def prepare_kernel(rows, *refs):
    chips = rows // 2
    mine, theirs, feat_hi, feat_lo, gate_ref = refs[:chips], *refs[chips : chips + 4]
    spect, opened = refs[chips + 4 :]
    order = order_rows(rows, gate_ref.shape[0])
    pieces = [(ref[0], theirs[zs]) for zs, ref in enumerate(mine)]
    for zs, part in enumerate(channel_part(order, pieces, feat_hi[...], feat_lo[...])):
        spect[zs] = part
    for start in range(0, gate_ref.shape[1], GROUP):
        cols = slice(start, start + GROUP)
        opened[:, cols] = jax.nn.sigmoid(gate_ref[:, cols].astype(jnp.float32))


def relay_kernel(first, second, to_first, to_second):
    rows = to_first.shape[0]
    to_first[...] = second[:rows, :]
    to_second[...] = first[rows:, :]


def final_kernel(rows, *refs):
    chips = rows // 2
    mine, feat_hi, feat_lo, spect, opened = refs[:chips], *refs[chips : chips + 4]
    w_mine, w_rest, *w_far, out_ref, lhs, result, sems = refs[chips + 4 :]
    count, width = opened.shape
    half = GROUP // 2
    row, col = lax.axis_index("row"), lax.axis_index("col")
    core, chip = row % 2, row // 2
    order = order_rows(rows, count)
    pieces = [(ref[0], ref[1]) for ref in mine]
    for zs, part in enumerate(channel_part(order, pieces, feat_hi[...], feat_lo[...])):
        whole = (part + spect[zs]).astype(jnp.bfloat16)
        for h in range(2):
            spot = pl.ds(pl.multiple_of((core ^ h) * half, half), half)
            lhs[zs, :, spot] = whole[:, h * half : (h + 1) * half]
    first, second, low, high = (w_far[i::4] for i in range(4))
    copies = []
    for t in range(width // GROUP):
        cols = slice(t * GROUP, (t + 1) * GROUP)
        total = jnp.zeros((count, GROUP), jnp.float32)
        for s in range(4):
            if s == 0:
                parts = [w_mine[:, cols], w_rest[:, cols]]
            elif s < 3:
                parts = [ref[:, cols] for ref in (first, second)[s - 1]]
            else:
                parts = [ref[:, cols] for pair in zip(low, high) for ref in pair]
            rhs = jnp.concatenate(parts, axis=0)
            total += jnp.dot(lhs[chip ^ col ^ s], rhs, preferred_element_type=jnp.float32)
        result[:, cols] = (opened[:, cols] * total).astype(jnp.bfloat16)
        copies.append(pltpu.make_async_copy(result.at[:, cols], out_ref.at[:, cols], sems.at[t]))
        copies[-1].start()
    for copy in copies:
        copy.wait()


def swap(value, axis, size, bit):
    return lax.ppermute(value, axis, [(i, i ^ bit) for i in range(size)])


def send_order(chips):
    return sorted(range(1, chips), key=lambda zs: (zs < 2, zs))


def across_chips(pieces, rows):
    chips = rows // 2
    got = [pieces[0]] + [None] * (chips - 1)
    for zs in send_order(chips):
        got[zs] = swap(pieces[zs], "row", rows, 2 * zs)
    return got


def on_device(mix_input, gate_logits, w_proj):
    return program(mix_input[0], gate_logits[0], w_proj)[None]


def program(tokens, gate, w_proj):
    count, features = tokens.shape
    rows, n_col = lax.axis_size("row"), lax.axis_size("col")
    chips = rows // 2
    lanes = features // (chips * CHUNKS)
    half = rows // 2
    width = w_proj.shape[1]
    scale = 1.0 / math.sqrt(count * rows * GROUP)
    table_hi, table_lo = split_halves(position_table(count, scale))
    twist = twist_table(rows, count)
    features_of = feature_table(lanes // 2)
    feat_hi, feat_lo = split_halves(features_of)
    bf = jnp.bfloat16
    fast = w_proj.shape[0] == GROUP and CHUNKS * lanes == GROUP and n_col == chips == 4

    half_w = jax.ShapeDtypeStruct((GROUP // 2, width), bf)
    picked = pl.pallas_call(
        functools.partial(pick_kernel, chips, fast),
        out_shape=[jax.ShapeDtypeStruct((CHUNKS, count, lanes), bf)] * chips
        + [half_w] * (2 * fast),
        in_specs=[pl.BlockSpec(memory_space=pl.ANY)] * 2,
        out_specs=[pl.BlockSpec(memory_space=pltpu.VMEM)] * (chips + 2 * fast),
        scratch_shapes=[
            pltpu.VMEM((chips, count, GROUP), bf),
            pltpu.SemaphoreType.DMA((chips,)),
            pltpu.SemaphoreType.DMA((2,)),
        ],
        compiler_params=pltpu.CompilerParams(vmem_limit_bytes=24 * MIB),
        cost_estimate=pl.CostEstimate(
            flops=2 * count * GROUP * features, bytes_accessed=MIB, transcendentals=0
        ),
    )(tokens, w_proj)
    arrived = across_chips(picked[:chips], rows)

    if fast:
        mine, rest = picked[chips:]
        w_own = []
        part = jax.ShapeDtypeStruct((GROUP // 4, width), bf)
        for s in (1, 2):
            w_own.append(swap(mine, "col", n_col, s))
        passed = vmem_call(relay_kernel, [part] * 2, [], GROUP * width, 2 * GROUP * width)(*w_own)
        for s in (1, 2):
            w_own.append(swap(passed[s - 1], "col", n_col, s))
        w_other = []
        for own in w_own:
            w_other.append(swap(own, "row", rows, 1))

    stacks = vmem_call(
        stack_kernel,
        [jax.ShapeDtypeStruct((chips, count, lanes), bf)] * CHUNKS,
        [],
        count * features,
        4 * count * features,
    )(*arrived)
    lines = half * (count // rows)
    piece = jax.ShapeDtypeStruct((2, lines, lanes), bf)
    stacked = jax.ShapeDtypeStruct((chips, lines, lanes), bf)
    small = (count * features // 4, count * features)
    sent = []
    for q in range(CHUNKS):
        theirs = swap(stacks[q], "row", rows, 1)
        sent.append(
            vmem_call(
                functools.partial(position_kernel, rows, q),
                [piece] * chips if q == 0 else [stacked] * 2,
                [
                    pltpu.VMEM((rows, count, lanes), jnp.float32),
                    pltpu.VMEM((2 * count, half * lanes), bf),
                    pltpu.VMEM((2 * count, half * lanes), bf),
                    pltpu.VMEM((half, count, lanes), jnp.float32),
                ],
                12 * count * count * half * lanes,
                rows * count * lanes * 4,
            )(*arrived, theirs, table_hi, table_lo, twist)
        )
    early = across_chips(sent[0], rows)
    give = vmem_call(give_kernel, stacked, [], *small)(*early)
    early.append(swap(give, "row", rows, 1))
    keep, give = sent[1]
    got = swap(give, "row", rows, 1)
    joined = vmem_call(join_kernel, [piece] * chips, [], *small)(keep, got)
    late = across_chips(joined, rows)
    if fast:
        spect, opened = vmem_call(
            functools.partial(prepare_kernel, rows),
            [
                jax.ShapeDtypeStruct((chips, count, GROUP), jnp.float32),
                jax.ShapeDtypeStruct((count, width), jnp.float32),
            ],
            [],
            2 * count * features * GROUP,
            6 * count * width,
        )(*early, feat_hi[0], feat_lo[0], gate)
        return pl.pallas_call(
            functools.partial(final_kernel, rows),
            out_shape=jax.ShapeDtypeStruct((count, width), bf),
            in_specs=[pl.BlockSpec(memory_space=pltpu.VMEM)] * (chips + 14),
            out_specs=pl.BlockSpec(memory_space=pl.ANY),
            scratch_shapes=[
                pltpu.VMEM((chips, count, GROUP), bf),
                pltpu.VMEM((count, width), bf),
                pltpu.SemaphoreType.DMA((width // GROUP,)),
            ],
            compiler_params=pltpu.CompilerParams(vmem_limit_bytes=32 * MIB),
            cost_estimate=pl.CostEstimate(
                flops=2 * count * features * width,
                bytes_accessed=2 * features * width,
                transcendentals=0,
            ),
        )(*late, feat_hi[1], feat_lo[1], spect, opened, mine, rest, *w_own, *w_other)

    weights = lax.all_gather(w_proj, "col", axis=0, tiled=True).reshape(-1, GROUP, width)
    order = order_rows(rows, count)
    chip = lax.axis_index("row") // 2
    table = jnp.asarray(features_of, jnp.float32).reshape(-1, CHUNKS, lanes, GROUP)
    per_group = table.shape[0]
    spectrum = jnp.zeros((count, weights.shape[0], GROUP), jnp.float32)
    here = chip ^ jnp.arange(chips)
    for q in range(CHUNKS):
        if q == 0:
            parts = [(early[zs][0], early[chips][zs]) for zs in range(chips)]
        else:
            parts = [(ref[0], ref[1]) for ref in late]
        got = jnp.stack([jnp.concatenate(pair, axis=0) for pair in parts])[here]
        got = jnp.einsum("kr,zrl->kzl", order, got, preferred_element_type=jnp.float32)
        spectrum += jnp.einsum(
            "kgtl,tlm->kgm",
            got.reshape(count, -1, per_group, lanes),
            table[:, q],
            precision=lax.Precision.HIGHEST,
        )
    total = jnp.einsum(
        "kgm,gmd->kd", spectrum.astype(bf), weights, preferred_element_type=jnp.float32
    )
    return (jax.nn.sigmoid(gate.astype(jnp.float32)) * total).astype(bf)


def solution(mesh):
    spec = P("col", "row", None)
    return jax.shard_map(
        on_device, mesh=mesh, in_specs=(spec, spec, P("col", None)), out_specs=spec, check_vma=False
    )
```

```python
import functools
import math

import jax
import jax.numpy as jnp
import numpy as np
from jax import lax
from jax.experimental import pallas as pl
from jax.experimental.pallas import tpu as pltpu
from jax.sharding import PartitionSpec as P


GROUP = 256
CHUNKS = 2
MIB = 1 << 20


def split_halves(table):
    head = table.astype(jnp.bfloat16)
    return head, (table - head.astype(np.float64)).astype(jnp.bfloat16)


def feature_table(pairs):
    chunks = GROUP // (2 * pairs)
    out = np.zeros((chunks, 2 * pairs, GROUP))
    m = np.arange(GROUP)
    for t in range(chunks):
        for j in range(pairs):
            c = pairs * t + j
            out[t, j] = np.cos(2 * math.pi * (m * c % GROUP) / GROUP)
            out[t, pairs + j] = -np.sin(2 * math.pi * (m * c % GROUP) / GROUP)
        if t == 0:
            out[0, pairs] = np.where(m % 2 == 0, 1.0, -1.0)
    return out


def position_table(inner, scale):
    angle = 2 * math.pi * (np.outer(np.arange(inner), np.arange(inner)) % inner) / inner
    return np.concatenate([np.cos(angle), np.sin(angle)], axis=1) * scale


def twist_table(rows, inner):
    length = rows * inner
    n2 = np.arange(inner)[:, None]
    res = []
    for core in range(2):
        k1 = 2 * np.arange(rows // 2)[None, :] + core
        angle = 2 * math.pi * (n2 * k1 % length) / length
        res.append(np.concatenate([np.cos(angle), np.sin(angle)], axis=1))
    return np.stack(res).astype(np.float32)


def vmem_call(body, outs, scratch, flops, moved, limit=24):
    return pl.pallas_call(
        body,
        out_shape=outs,
        scratch_shapes=scratch,
        compiler_params=pltpu.CompilerParams(vmem_limit_bytes=limit * MIB),
        cost_estimate=pl.CostEstimate(flops=flops, bytes_accessed=moved, transcendentals=0),
    )


def pick_kernel(chips, fast, *refs):
    x_ref, w_ref = refs[:2]
    outs = [refs[2 + q * chips : 2 + (q + 1) * chips] for q in range(CHUNKS)]
    halves = refs[2 + CHUNKS * chips : -3]
    tokens, x_sems, w_sems = refs[-3:]
    row = lax.axis_index("row")
    core, chip = row % 2, row // 2
    lanes = outs[0][0].shape[1]
    pairs = lanes // 2
    chips_per_group = GROUP // (CHUNKS * lanes)
    loads = []
    for zs in range(chips):
        group = (chip ^ zs) // chips_per_group
        columns = pl.ds(pl.multiple_of(group * GROUP, GROUP), GROUP)
        loads.append(pltpu.make_async_copy(x_ref.at[:, columns], tokens.at[zs], x_sems.at[zs]))
    order = [*send_order(chips), 0]
    for zs in order:
        loads[zs].start()
    fetches = []
    if fast:
        half = GROUP // 2
        for i, h in enumerate((core, 1 - core)):
            part = w_ref.at[pl.ds(pl.multiple_of(h * half, half), half), :]
            fetches.append(pltpu.make_async_copy(part, halves[i], w_sems.at[i]))
            fetches[-1].start()
    src = lax.broadcasted_iota(jnp.int32, (GROUP, CHUNKS * lanes), 0)
    column = lax.broadcasted_iota(jnp.int32, (GROUP, CHUNKS * lanes), 1)
    lane, j = column % lanes, column % lanes - pairs
    for zs in order:
        part = ((chip ^ zs) % chips_per_group) * CHUNKS + column // lanes
        mirrored = jnp.where((j == 0) & (part == 0), GROUP // 2, GROUP - pairs * part - j)
        wanted = jnp.where(lane < pairs, pairs * part + lane, mirrored)
        choose = (src == wanted).astype(jnp.bfloat16)
        loads[zs].wait()
        got = jnp.dot(tokens[zs], choose, preferred_element_type=jnp.float32).astype(jnp.bfloat16)
        for q in range(CHUNKS):
            outs[q][zs][...] = got[:, q * lanes : (q + 1) * lanes]
    for fetch in fetches:
        fetch.wait()


def stack_kernel(*refs):
    for zs, piece in enumerate(refs[:-1]):
        refs[-1][zs] = piece[...]


def complex_dft(values):
    n = len(values)
    if n == 1:
        return values
    even, odd = complex_dft(values[0::2]), complex_dft(values[1::2])
    low, high = [], []
    for k in range(n // 2):
        c, s = math.cos(2 * math.pi * k / n), math.sin(2 * math.pi * k / n)
        re, im = odd[k]
        if k == 0:
            tr, ti = re, im
        elif 4 * k == n:
            tr, ti = im, -re
        else:
            tr, ti = re * c + im * s, im * c - re * s
        er, ei = even[k]
        low.append((er + tr, ei + ti))
        high.append((er - tr, ei - ti))
    return low + high


def position_kernel(rows, q, *refs):
    chips = rows // 2
    mine, theirs = refs[:chips], refs[chips]
    table, twist = refs[chips + 1 : chips + 3]
    *outs, folded, turned_z, spect = refs[chips + 3 :]
    inner, lanes = mine[0].shape
    pairs = lanes // 2
    row = lax.axis_index("row")
    core, chip = row % 2, row // 2
    half = rows // 2

    lane = lax.broadcasted_iota(jnp.int32, (1, lanes), 1)
    chips_per_group = GROUP // (CHUNKS * lanes)
    first = (chip % chips_per_group == 0) if q == 0 else False
    lone_low = (lane == 0) & first
    lone_high = (lane == pairs) & first
    own = jnp.where((lane < pairs) | lone_high, 1.0, -1.0).astype(jnp.float32)
    other = jnp.where(lone_low | lone_high, 0.0, 1.0).astype(jnp.float32)
    cosine = (lane < pairs) | lone_high

    def fold(block):
        value = block.astype(jnp.float32)
        if lanes % 128 == 0:
            turned = pltpu.roll(value, pairs, 1)
        else:
            turned = jnp.concatenate([value[:, pairs:], value[:, :pairs]], axis=1)
        return value * own + turned * other

    for zs in range(chips):
        folded[row ^ (2 * zs)] = fold(mine[zs][...])
        folded[row ^ (2 * zs + 1)] = fold(theirs[zs])

    odd_core = core == 1
    sign = jnp.where(odd_core, -1.0, 1.0).astype(jnp.float32)
    turns = []
    for n in range(half):
        angle = 2 * math.pi * n / rows
        turns.append(
            (
                jnp.where(odd_core, math.cos(angle), 1.0).astype(jnp.float32),
                jnp.where(odd_core, -math.sin(angle), 0.0).astype(jnp.float32),
            )
        )
    tile = min(inner, 32)

    def step(i, carry):
        at = pl.ds(pl.multiple_of(i * tile, tile), tile)
        low_at = pl.ds(pl.multiple_of(inner + i * tile, tile), tile)
        values = []
        for n in range(half):
            v = folded[n, at, :] + sign * folded[n + half, at, :]
            values.append((v * turns[n][0], v * turns[n][1]))
        tw = twist[core, at, :]
        for j, (re, im) in enumerate(complex_dft(values)):
            a = jnp.where(cosine, re, -im)
            b = jnp.where(cosine, im, re)
            c, s = tw[:, j : j + 1], tw[:, half + j : half + j + 1]
            for where, z in ((at, a * c + b * s), (low_at, b * c - a * s)):
                turned_z[where, j * lanes : (j + 1) * lanes] = z.astype(jnp.bfloat16)
        return carry

    lax.fori_loop(0, inner // tile, step, 0)
    width = min(half * lanes, 256)
    for start in range(0, half * lanes, width):
        cols = slice(start, start + width)
        value = jnp.dot(table[...], turned_z[:, cols], preferred_element_type=jnp.float32)
        for j in range(start // lanes, (start + width) // lanes):
            piece = value[:, j * lanes - start : (j + 1) * lanes - start]
            spect[j] = piece
    per = inner // rows
    for zs in range(chips):
        for rel in range(2):
            dest = row ^ (2 * zs + rel)
            for j in range(half):
                piece = spect[j, pl.ds(pl.multiple_of(dest * per, per), per), :]
                outs[zs][rel, j * per : (j + 1) * per, :] = piece.astype(jnp.bfloat16)


def order_rows(rows, count):
    core = lax.axis_index("row") % 2
    half, per = rows // 2, count // rows
    natural = lax.broadcasted_iota(jnp.int32, (count, count), 0)
    received = lax.broadcasted_iota(jnp.int32, (count, count), 1)
    rel, j, k2 = received // (half * per), received // per % half, received % per
    return (natural == rows * k2 + 2 * j + (core ^ rel)).astype(jnp.bfloat16)


def give_kernel(*refs):
    out = refs[-1]
    for zs, ref in enumerate(refs[:-1]):
        out[zs] = ref[1]


def join_kernel(first, second, out):
    out[0] = first[...]
    out[1] = second[...]


def channel_part(order, pieces, feat_hi, feat_lo):
    lanes = feat_hi.shape[0]
    got = jnp.concatenate([jnp.concatenate(piece, axis=0) for piece in pieces], axis=1)
    got = jnp.dot(order, got, preferred_element_type=jnp.float32).astype(jnp.bfloat16)
    parts = []
    for zs in range(len(pieces)):
        piece = got[:, zs * lanes : (zs + 1) * lanes]
        part = jnp.dot(piece, feat_hi, preferred_element_type=jnp.float32)
        parts.append(part + jnp.dot(piece, feat_lo, preferred_element_type=jnp.float32))
    return parts


def prepare_kernel(rows, *refs):
    chips = rows // 2
    mine, theirs, feat_hi, feat_lo, gate_ref = refs[:chips], *refs[chips : chips + 4]
    spect, opened = refs[chips + 4 :]
    order = order_rows(rows, gate_ref.shape[0])
    pieces = [(ref[0], theirs[zs]) for zs, ref in enumerate(mine)]
    for zs, part in enumerate(channel_part(order, pieces, feat_hi[...], feat_lo[...])):
        spect[zs] = part
    for start in range(0, gate_ref.shape[1], GROUP):
        cols = slice(start, start + GROUP)
        opened[:, cols] = jax.nn.sigmoid(gate_ref[:, cols].astype(jnp.float32))


def final_kernel(rows, *refs):
    chips = rows // 2
    mine, theirs, feat_hi, feat_lo, spect, opened = refs[:chips], *refs[chips : chips + 5]
    w_mine, w_rest, w_a, w_b, v_a, v_b, out_ref, lhs, result, sems = refs[chips + 5 :]
    count, width = opened.shape
    half = GROUP // 2
    row, col = lax.axis_index("row"), lax.axis_index("col")
    core, chip = row % 2, row // 2
    order = order_rows(rows, count)
    pieces = [(ref[0], theirs[zs]) for zs, ref in enumerate(mine)]
    for zs, part in enumerate(channel_part(order, pieces, feat_hi[...], feat_lo[...])):
        whole = (part + spect[zs]).astype(jnp.bfloat16)
        for h in range(2):
            spot = pl.ds(pl.multiple_of((core ^ h) * half, half), half)
            lhs[zs, :, spot] = whole[:, h * half : (h + 1) * half]
    weights = (
        (0, lambda at: (w_mine[:, at], w_rest[:, at])),
        (1 + core, lambda at: (w_a[:, at], v_b[0, :, at])),
        (2 - core, lambda at: (w_b[0, :, at], v_a[:, at])),
        (3, lambda at: (w_b[1, :, at], v_b[1, :, at])),
    )
    copies = []
    for t in range(width // GROUP):
        cols = slice(t * GROUP, (t + 1) * GROUP)
        total = jnp.zeros((count, GROUP), jnp.float32)
        for s, halves in weights:
            rhs = jnp.concatenate(halves(cols), axis=0)
            total += jnp.dot(lhs[chip ^ col ^ s], rhs, preferred_element_type=jnp.float32)
        result[:, cols] = (opened[:, cols] * total).astype(jnp.bfloat16)
        copies.append(pltpu.make_async_copy(result.at[:, cols], out_ref.at[:, cols], sems.at[t]))
        copies[-1].start()
    for copy in copies:
        copy.wait()


def swap(value, axis, size, bit):
    return lax.ppermute(value, axis, [(i, i ^ bit) for i in range(size)])


def turn_swap(value, rows, n_col, bits):
    turn = [
        (row * n_col + col, row * n_col + (col ^ bits[row % 2]))
        for row in range(rows)
        for col in range(n_col)
    ]
    return lax.ppermute(value, ("row", "col"), turn)


def send_order(chips):
    return sorted(range(1, chips), key=lambda zs: (zs < 2, zs))


def across_chips(pieces, rows):
    chips = rows // 2
    got = [pieces[0]] + [None] * (chips - 1)
    for zs in send_order(chips):
        got[zs] = swap(pieces[zs], "row", rows, 2 * zs)
    return got


def on_device(mix_input, gate_logits, w_proj):
    return program(mix_input[0], gate_logits[0], w_proj)[None]


def program(tokens, gate, w_proj):
    count, features = tokens.shape
    rows, n_col = lax.axis_size("row"), lax.axis_size("col")
    chips = rows // 2
    lanes = features // (chips * CHUNKS)
    half = rows // 2
    width = w_proj.shape[1]
    scale = 1.0 / math.sqrt(count * rows * GROUP)
    table = position_table(count, scale).astype(jnp.bfloat16)
    twist = twist_table(rows, count)
    features_of = feature_table(lanes // 2)
    feat_hi, feat_lo = split_halves(features_of)
    bf = jnp.bfloat16
    fast = w_proj.shape[0] == GROUP and CHUNKS * lanes == GROUP and n_col == chips == 4

    half_w = jax.ShapeDtypeStruct((GROUP // 2, width), bf)
    picked = pl.pallas_call(
        functools.partial(pick_kernel, chips, fast),
        out_shape=[jax.ShapeDtypeStruct((count, lanes), bf)] * (CHUNKS * chips)
        + [half_w] * (2 * fast),
        in_specs=[pl.BlockSpec(memory_space=pltpu.HBM)] * 2,
        out_specs=[pl.BlockSpec(memory_space=pltpu.VMEM)] * (CHUNKS * chips + 2 * fast),
        scratch_shapes=[
            pltpu.VMEM((chips, count, GROUP), bf),
            pltpu.SemaphoreType.DMA((chips,)),
            pltpu.SemaphoreType.DMA((2,)),
        ],
        compiler_params=pltpu.CompilerParams(vmem_limit_bytes=24 * MIB),
        cost_estimate=pl.CostEstimate(
            flops=2 * count * GROUP * features, bytes_accessed=MIB, transcendentals=0
        ),
    )(*(pltpu.with_memory_space_constraint(v, pltpu.HBM) for v in (tokens, w_proj)))
    arrived = [across_chips(picked[q * chips : (q + 1) * chips], rows) for q in range(CHUNKS)]

    if fast:
        mine, rest = picked[CHUNKS * chips :]
        w_a = turn_swap(mine, rows, n_col, (1, 2))
        pair = vmem_call(
            join_kernel,
            jax.ShapeDtypeStruct((2, GROUP // 2, width), bf),
            [],
            GROUP * width,
            4 * GROUP * width,
        )(mine, w_a)
        w_b = turn_swap(pair, rows, n_col, (2, 1))
        v_a = swap(w_a, "row", rows, 1)
        v_b = swap(w_b, "row", rows, 1)

    lines = half * (count // rows)
    piece = jax.ShapeDtypeStruct((2, lines, lanes), bf)
    small = (count * features // 4, count * features)
    received = []
    for q in range(CHUNKS):
        stack = vmem_call(
            stack_kernel, jax.ShapeDtypeStruct((chips, count, lanes), bf), [], *small
        )(*arrived[q])
        theirs = swap(stack, "row", rows, 1)
        sent = vmem_call(
            functools.partial(position_kernel, rows, q),
            [piece] * chips,
            [
                pltpu.VMEM((rows, count, lanes), jnp.float32),
                pltpu.VMEM((2 * count, half * lanes), bf),
                pltpu.VMEM((half, count, lanes), jnp.float32),
            ],
            4 * count * count * half * lanes,
            rows * count * lanes * 4,
        )(*arrived[q], theirs, table, twist)
        got = across_chips(sent, rows)
        give = vmem_call(
            give_kernel, jax.ShapeDtypeStruct((chips, lines, lanes), bf), [], *small
        )(*got)
        got.append(swap(give, "row", rows, 1))
        received.append(got)
    early, late = received
    if fast:
        spect, opened = vmem_call(
            functools.partial(prepare_kernel, rows),
            [
                jax.ShapeDtypeStruct((chips, count, GROUP), jnp.float32),
                jax.ShapeDtypeStruct((count, width), jnp.float32),
            ],
            [],
            2 * count * features * GROUP,
            6 * count * width,
        )(*early, feat_hi[0], feat_lo[0], gate)
        return pl.pallas_call(
            functools.partial(final_kernel, rows),
            out_shape=jax.ShapeDtypeStruct((count, width), bf),
            in_specs=[pl.BlockSpec(memory_space=pltpu.VMEM)] * (chips + 11),
            out_specs=pl.BlockSpec(memory_space=pl.ANY),
            scratch_shapes=[
                pltpu.VMEM((chips, count, GROUP), bf),
                pltpu.VMEM((count, width), bf),
                pltpu.SemaphoreType.DMA((width // GROUP,)),
            ],
            compiler_params=pltpu.CompilerParams(vmem_limit_bytes=32 * MIB),
            cost_estimate=pl.CostEstimate(
                flops=2 * count * features * width,
                bytes_accessed=2 * features * width,
                transcendentals=0,
            ),
        )(*late, feat_hi[1], feat_lo[1], spect, opened, mine, rest, w_a, w_b, v_a, v_b)

    weights = lax.all_gather(w_proj, "col", axis=0, tiled=True).reshape(-1, GROUP, width)
    order = order_rows(rows, count)
    chip = lax.axis_index("row") // 2
    table = jnp.asarray(features_of, jnp.float32).reshape(-1, CHUNKS, lanes, GROUP)
    per_group = table.shape[0]
    spectrum = jnp.zeros((count, weights.shape[0], GROUP), jnp.float32)
    here = chip ^ jnp.arange(chips)
    for q in range(CHUNKS):
        parts = [(received[q][zs][0], received[q][chips][zs]) for zs in range(chips)]
        got = jnp.stack([jnp.concatenate(pair, axis=0) for pair in parts])[here]
        got = jnp.einsum("kr,zrl->kzl", order, got, preferred_element_type=jnp.float32)
        spectrum += jnp.einsum(
            "kgtl,tlm->kgm",
            got.reshape(count, -1, per_group, lanes),
            table[:, q],
            precision=lax.Precision.HIGHEST,
        )
    total = jnp.einsum(
        "kgm,gmd->kd", spectrum.astype(bf), weights, preferred_element_type=jnp.float32
    )
    return (jax.nn.sigmoid(gate.astype(jnp.float32)) * total).astype(bf)


def solution(mesh):
    spec = P("col", "row", None)
    return jax.shard_map(
        on_device, mesh=mesh, in_specs=(spec, spec, P("col", None)), out_specs=spec, check_vma=False
    )
```

```python
import functools
import math

import jax
import jax.numpy as jnp
import numpy as np
from jax import lax
from jax.experimental import pallas as pl
from jax.experimental.pallas import tpu as pltpu
from jax.sharding import PartitionSpec as P


GROUP = 256
CHUNKS = 2
MIB = 1 << 20


def split_halves(table):
    head = table.astype(jnp.bfloat16)
    return head, (table - head.astype(np.float64)).astype(jnp.bfloat16)


def feature_table(pairs):
    chunks = GROUP // (2 * pairs)
    out = np.zeros((chunks, 2 * pairs, GROUP))
    m = np.arange(GROUP)
    for t in range(chunks):
        for j in range(pairs):
            c = pairs * t + j
            out[t, j] = np.cos(2 * math.pi * (m * c % GROUP) / GROUP)
            out[t, pairs + j] = -np.sin(2 * math.pi * (m * c % GROUP) / GROUP)
        if t == 0:
            out[0, pairs] = np.where(m % 2 == 0, 1.0, -1.0)
    return out


def position_table(inner, scale):
    angle = 2 * math.pi * (np.outer(np.arange(inner), np.arange(inner)) % inner) / inner
    return np.concatenate([np.cos(angle), np.sin(angle)], axis=1) * scale


def twist_table(rows, inner):
    length = rows * inner
    n2 = np.arange(inner)[:, None]
    res = []
    for core in range(2):
        k1 = 2 * np.arange(rows // 2)[None, :] + core
        angle = 2 * math.pi * (n2 * k1 % length) / length
        res.append(np.concatenate([np.cos(angle), np.sin(angle)], axis=1))
    return np.stack(res).astype(np.float32)


def vmem_call(body, outs, scratch, flops, moved, limit=24):
    return pl.pallas_call(
        body,
        out_shape=outs,
        scratch_shapes=scratch,
        compiler_params=pltpu.CompilerParams(vmem_limit_bytes=limit * MIB),
        cost_estimate=pl.CostEstimate(flops=flops, bytes_accessed=moved, transcendentals=0),
    )


def pick_kernel(chips, fast, *refs):
    x_ref, w_ref = refs[:2]
    outs = [refs[2 + q * chips : 2 + (q + 1) * chips] for q in range(CHUNKS)]
    halves = refs[2 + CHUNKS * chips : -3]
    tokens, x_sems, w_sems = refs[-3:]
    row = lax.axis_index("row")
    core, chip = row % 2, row // 2
    lanes = outs[0][0].shape[1]
    pairs = lanes // 2
    chips_per_group = GROUP // (CHUNKS * lanes)
    loads = []
    for zs in range(chips):
        group = (chip ^ zs) // chips_per_group
        columns = pl.ds(pl.multiple_of(group * GROUP, GROUP), GROUP)
        loads.append(pltpu.make_async_copy(x_ref.at[:, columns], tokens.at[zs], x_sems.at[zs]))
    order = [*send_order(chips), 0]
    for zs in order:
        loads[zs].start()
    fetches = []
    if fast:
        half = GROUP // 2
        for i, h in enumerate((core, 1 - core)):
            part = w_ref.at[pl.ds(pl.multiple_of(h * half, half), half), :]
            fetches.append(pltpu.make_async_copy(part, halves[i], w_sems.at[i]))
            fetches[-1].start()
    src = lax.broadcasted_iota(jnp.int32, (GROUP, CHUNKS * lanes), 0)
    column = lax.broadcasted_iota(jnp.int32, (GROUP, CHUNKS * lanes), 1)
    lane, j = column % lanes, column % lanes - pairs
    choose = None
    for zs in order:
        if choose is None or chips_per_group > 1:
            part = ((chip ^ zs) % chips_per_group) * CHUNKS + column // lanes
            mirrored = jnp.where((j == 0) & (part == 0), GROUP // 2, GROUP - pairs * part - j)
            wanted = jnp.where(lane < pairs, pairs * part + lane, mirrored)
            choose = (src == wanted).astype(jnp.bfloat16)
        loads[zs].wait()
        got = jnp.dot(tokens[zs], choose, preferred_element_type=jnp.float32).astype(jnp.bfloat16)
        for q in range(CHUNKS):
            outs[q][zs][...] = got[:, q * lanes : (q + 1) * lanes]
    for fetch in fetches:
        fetch.wait()


def stack_kernel(*refs):
    for zs, piece in enumerate(refs[:-1]):
        refs[-1][zs] = piece[...]


def complex_dft(values):
    n = len(values)
    if n == 1:
        return values
    even, odd = complex_dft(values[0::2]), complex_dft(values[1::2])
    low, high = [], []
    for k in range(n // 2):
        c, s = math.cos(2 * math.pi * k / n), math.sin(2 * math.pi * k / n)
        re, im = odd[k]
        if k == 0:
            tr, ti = re, im
        elif 4 * k == n:
            tr, ti = im, -re
        else:
            tr, ti = re * c + im * s, im * c - re * s
        er, ei = even[k]
        low.append((er + tr, ei + ti))
        high.append((er - tr, ei - ti))
    return low + high


def position_kernel(rows, q, *refs):
    chips = rows // 2
    mine, theirs = refs[:chips], refs[chips]
    table_hi, table_lo, twist = refs[chips + 1 : chips + 4]
    *outs, folded, turned_z, spect = refs[chips + 4 :]
    inner, lanes = mine[0].shape
    pairs = lanes // 2
    row = lax.axis_index("row")
    core, chip = row % 2, row // 2
    half = rows // 2

    lane = lax.broadcasted_iota(jnp.int32, (1, lanes), 1)
    chips_per_group = GROUP // (CHUNKS * lanes)
    first = (chip % chips_per_group == 0) if q == 0 else False
    lone_low = (lane == 0) & first
    lone_high = (lane == pairs) & first
    own = jnp.where((lane < pairs) | lone_high, 1.0, -1.0).astype(jnp.float32)
    other = jnp.where(lone_low | lone_high, 0.0, 1.0).astype(jnp.float32)
    cosine = (lane < pairs) | lone_high

    odd_core = core == 1
    sign = jnp.where(odd_core, -1.0, 1.0).astype(jnp.float32)
    upper = row >= half
    near, far = jnp.where(upper, sign, 1.0), jnp.where(upper, 1.0, sign)

    def block(s):
        value = mine[s // 2][...] if s % 2 == 0 else theirs[s // 2]
        return value.astype(jnp.float32)

    for s in range(half):
        value = near * block(s) + far * block(s ^ half)
        if lanes % 128 == 0:
            rolled = pltpu.roll(value, pairs, 1)
        else:
            rolled = jnp.concatenate([value[:, pairs:], value[:, :pairs]], axis=1)
        folded[(row % half) ^ s] = value * own + rolled * other

    turns = []
    for n in range(half):
        angle = 2 * math.pi * n / rows
        c = jnp.where(odd_core, math.cos(angle), 1.0).astype(jnp.float32)
        d = jnp.where(odd_core, math.sin(angle), 0.0).astype(jnp.float32)
        turns.append((jnp.where(cosine, c, d), jnp.where(cosine, -d, c)))
    tile = min(inner, 32)

    def step(i, carry):
        at = pl.ds(pl.multiple_of(i * tile, tile), tile)
        low_at = pl.ds(pl.multiple_of(inner + i * tile, tile), tile)
        values = []
        for n in range(half):
            v = folded[n, at, :]
            values.append((v * turns[n][0], v * turns[n][1]))
        tw = twist[core, at, :]
        for j, (a, b) in enumerate(complex_dft(values)):
            c, s = tw[:, j : j + 1], tw[:, half + j : half + j + 1]
            cols = slice(j * lanes, (j + 1) * lanes)
            turned_z[at, cols] = (a * c + b * s).astype(jnp.bfloat16)
            turned_z[low_at, cols] = (b * c - a * s).astype(jnp.bfloat16)
        return carry

    lax.fori_loop(0, inner // tile, step, 0)
    width = min(half * lanes, 256)
    for start in range(0, half * lanes, width):
        cols = slice(start, start + width)
        value = jnp.dot(table_hi[...], turned_z[:, cols], preferred_element_type=jnp.float32)
        value += jnp.dot(table_lo[...], turned_z[:, cols], preferred_element_type=jnp.float32)
        for j in range(start // lanes, (start + width) // lanes):
            piece = value[:, j * lanes - start : (j + 1) * lanes - start]
            spect[j] = piece
    per = inner // rows
    for zs in range(chips):
        for rel in range(2):
            dest = row ^ (2 * zs + rel)
            for j in range(half):
                piece = spect[j, pl.ds(pl.multiple_of(dest * per, per), per), :]
                lines = slice(j * per, (j + 1) * per)
                if q == 0:
                    outs[zs][rel, lines, :] = piece.astype(jnp.bfloat16)
                else:
                    outs[rel][zs, lines, :] = piece.astype(jnp.bfloat16)


def order_rows(rows, count):
    core = lax.axis_index("row") % 2
    half, per = rows // 2, count // rows
    natural = lax.broadcasted_iota(jnp.int32, (count, count), 0)
    received = lax.broadcasted_iota(jnp.int32, (count, count), 1)
    rel, j, k2 = received // (half * per), received // per % half, received % per
    return (natural == rows * k2 + 2 * j + (core ^ rel)).astype(jnp.bfloat16)


def give_kernel(*refs):
    out = refs[-1]
    for zs, ref in enumerate(refs[:-1]):
        out[zs] = ref[1]


def join_kernel(keep, got, *outs):
    for zs, out in enumerate(outs):
        out[0] = keep[zs]
        out[1] = got[zs]


def channel_part(order, pieces, feat_hi, feat_lo):
    lanes = feat_hi.shape[0]
    got = jnp.concatenate([jnp.concatenate(piece, axis=0) for piece in pieces], axis=1)
    got = jnp.dot(order, got, preferred_element_type=jnp.float32).astype(jnp.bfloat16)
    parts = []
    for zs in range(len(pieces)):
        piece = got[:, zs * lanes : (zs + 1) * lanes]
        part = jnp.dot(piece, feat_hi, preferred_element_type=jnp.float32)
        parts.append(part + jnp.dot(piece, feat_lo, preferred_element_type=jnp.float32))
    return parts


def prepare_kernel(rows, *refs):
    chips = rows // 2
    mine, theirs, feat_hi, feat_lo, gate_ref = refs[:chips], *refs[chips : chips + 4]
    spect, opened = refs[chips + 4 :]
    order = order_rows(rows, gate_ref.shape[0])
    pieces = [(ref[0], theirs[zs]) for zs, ref in enumerate(mine)]
    for zs, part in enumerate(channel_part(order, pieces, feat_hi[...], feat_lo[...])):
        spect[zs] = part
    for start in range(0, gate_ref.shape[1], GROUP):
        cols = slice(start, start + GROUP)
        opened[:, cols] = jax.nn.sigmoid(gate_ref[:, cols].astype(jnp.float32))


def final_kernel(rows, *refs):
    chips = rows // 2
    mine, feat_hi, feat_lo, spect, opened = refs[:chips], *refs[chips : chips + 4]
    w_mine, w_rest, w_a, w_b, w_c, v_a, v_b, v_c, out_ref, lhs, result, sems = refs[chips + 4 :]
    count, width = opened.shape
    half = GROUP // 2
    row, col = lax.axis_index("row"), lax.axis_index("col")
    core, chip = row % 2, row // 2
    order = order_rows(rows, count)
    pieces = [(ref[0], ref[1]) for ref in mine]
    for zs, part in enumerate(channel_part(order, pieces, feat_hi[...], feat_lo[...])):
        whole = (part + spect[zs]).astype(jnp.bfloat16)
        for h in range(2):
            spot = pl.ds(pl.multiple_of((core ^ h) * half, half), half)
            lhs[zs, :, spot] = whole[:, h * half : (h + 1) * half]
    weights = (
        (0, w_mine, w_rest),
        (1 + core, w_a, v_b),
        (2 - core, w_b, v_a),
        (3, w_c, v_c),
    )
    copies = []
    for t in range(width // GROUP):
        cols = slice(t * GROUP, (t + 1) * GROUP)
        total = jnp.zeros((count, GROUP), jnp.float32)
        for s, w_here, w_there in weights:
            rhs = jnp.concatenate([w_here[:, cols], w_there[:, cols]], axis=0)
            total += jnp.dot(lhs[chip ^ col ^ s], rhs, preferred_element_type=jnp.float32)
        result[:, cols] = (opened[:, cols] * total).astype(jnp.bfloat16)
        copies.append(pltpu.make_async_copy(result.at[:, cols], out_ref.at[:, cols], sems.at[t]))
        copies[-1].start()
    for copy in copies:
        copy.wait()


def swap(value, axis, size, bit):
    return lax.ppermute(value, axis, [(i, i ^ bit) for i in range(size)])


def turn_swap(value, rows, n_col, bits):
    turn = [
        (row * n_col + col, row * n_col + (col ^ bits[row % 2]))
        for row in range(rows)
        for col in range(n_col)
    ]
    return lax.ppermute(value, ("row", "col"), turn)


def send_order(chips):
    return sorted(range(1, chips), key=lambda zs: (zs < 2, zs))


def across_chips(pieces, rows):
    chips = rows // 2
    got = [pieces[0]] + [None] * (chips - 1)
    for zs in send_order(chips):
        got[zs] = swap(pieces[zs], "row", rows, 2 * zs)
    return got


def on_device(mix_input, gate_logits, w_proj):
    return program(mix_input[0], gate_logits[0], w_proj)[None]


def program(tokens, gate, w_proj):
    count, features = tokens.shape
    rows, n_col = lax.axis_size("row"), lax.axis_size("col")
    chips = rows // 2
    lanes = features // (chips * CHUNKS)
    half = rows // 2
    width = w_proj.shape[1]
    scale = 1.0 / math.sqrt(count * rows * GROUP)
    table_hi, table_lo = split_halves(position_table(count, scale))
    twist = twist_table(rows, count)
    features_of = feature_table(lanes // 2)
    feat_hi, feat_lo = split_halves(features_of)
    bf = jnp.bfloat16
    fast = w_proj.shape[0] == GROUP and CHUNKS * lanes == GROUP and n_col == chips == 4

    half_w = jax.ShapeDtypeStruct((GROUP // 2, width), bf)
    picked = pl.pallas_call(
        functools.partial(pick_kernel, chips, fast),
        out_shape=[jax.ShapeDtypeStruct((count, lanes), bf)] * (CHUNKS * chips)
        + [half_w] * (2 * fast),
        in_specs=[pl.BlockSpec(memory_space=pltpu.HBM)] * 2,
        out_specs=[pl.BlockSpec(memory_space=pltpu.VMEM)] * (CHUNKS * chips + 2 * fast),
        scratch_shapes=[
            pltpu.VMEM((chips, count, GROUP), bf),
            pltpu.SemaphoreType.DMA((chips,)),
            pltpu.SemaphoreType.DMA((2,)),
        ],
        compiler_params=pltpu.CompilerParams(vmem_limit_bytes=24 * MIB),
        cost_estimate=pl.CostEstimate(
            flops=2 * count * GROUP * features, bytes_accessed=MIB, transcendentals=0
        ),
    )(*(pltpu.with_memory_space_constraint(v, pltpu.HBM) for v in (tokens, w_proj)))
    arrived = [across_chips(picked[q * chips : (q + 1) * chips], rows) for q in range(CHUNKS)]

    if fast:
        mine, rest = picked[CHUNKS * chips :]
        w_a = turn_swap(mine, rows, n_col, (1, 2))
        w_b = turn_swap(mine, rows, n_col, (2, 1))
        w_c = turn_swap(w_a, rows, n_col, (2, 1))
        others = []
        for own in (w_a, w_b, w_c):
            others.append(swap(own, "row", rows, 1))

    lines = half * (count // rows)
    piece = jax.ShapeDtypeStruct((2, lines, lanes), bf)
    small = (count * features // 4, count * features)
    stacked = jax.ShapeDtypeStruct((chips, lines, lanes), bf)
    sent = []
    for q in range(CHUNKS):
        stack = vmem_call(
            stack_kernel, jax.ShapeDtypeStruct((chips, count, lanes), bf), [], *small
        )(*arrived[q])
        theirs = swap(stack, "row", rows, 1)
        sent.append(
            vmem_call(
                functools.partial(position_kernel, rows, q),
                [piece] * chips if q == 0 else [stacked] * 2,
                [
                    pltpu.VMEM((half, count, lanes), jnp.float32),
                    pltpu.VMEM((2 * count, half * lanes), bf),
                    pltpu.VMEM((half, count, lanes), jnp.float32),
                ],
                8 * count * count * half * lanes,
                rows * count * lanes * 4,
            )(*arrived[q], theirs, table_hi, table_lo, twist)
        )
    early = across_chips(sent[0], rows)
    give = vmem_call(give_kernel, stacked, [], *small)(*early)
    early.append(swap(give, "row", rows, 1))
    keep, give = sent[1]
    got = swap(give, "row", rows, 1)
    joined = vmem_call(join_kernel, [piece] * chips, [], *small)(keep, got)
    late = across_chips(joined, rows)
    if fast:
        spect, opened = vmem_call(
            functools.partial(prepare_kernel, rows),
            [
                jax.ShapeDtypeStruct((chips, count, GROUP), jnp.float32),
                jax.ShapeDtypeStruct((count, width), jnp.float32),
            ],
            [],
            2 * count * features * GROUP,
            6 * count * width,
        )(*early, feat_hi[0], feat_lo[0], gate)
        return pl.pallas_call(
            functools.partial(final_kernel, rows),
            out_shape=jax.ShapeDtypeStruct((count, width), bf),
            in_specs=[pl.BlockSpec(memory_space=pltpu.VMEM)] * (chips + 12),
            out_specs=pl.BlockSpec(memory_space=pl.ANY),
            scratch_shapes=[
                pltpu.VMEM((chips, count, GROUP), bf),
                pltpu.VMEM((count, width), bf),
                pltpu.SemaphoreType.DMA((width // GROUP,)),
            ],
            compiler_params=pltpu.CompilerParams(vmem_limit_bytes=32 * MIB),
            cost_estimate=pl.CostEstimate(
                flops=2 * count * features * width,
                bytes_accessed=2 * features * width,
                transcendentals=0,
            ),
        )(*late, feat_hi[1], feat_lo[1], spect, opened, mine, rest, w_a, w_b, w_c, *others)

    weights = lax.all_gather(w_proj, "col", axis=0, tiled=True).reshape(-1, GROUP, width)
    order = order_rows(rows, count)
    chip = lax.axis_index("row") // 2
    table = jnp.asarray(features_of, jnp.float32).reshape(-1, CHUNKS, lanes, GROUP)
    per_group = table.shape[0]
    spectrum = jnp.zeros((count, weights.shape[0], GROUP), jnp.float32)
    here = chip ^ jnp.arange(chips)
    for q in range(CHUNKS):
        if q == 0:
            parts = [(early[zs][0], early[chips][zs]) for zs in range(chips)]
        else:
            parts = [(ref[0], ref[1]) for ref in late]
        got = jnp.stack([jnp.concatenate(pair, axis=0) for pair in parts])[here]
        got = jnp.einsum("kr,zrl->kzl", order, got, preferred_element_type=jnp.float32)
        spectrum += jnp.einsum(
            "kgtl,tlm->kgm",
            got.reshape(count, -1, per_group, lanes),
            table[:, q],
            precision=lax.Precision.HIGHEST,
        )
    total = jnp.einsum(
        "kgm,gmd->kd", spectrum.astype(bf), weights, preferred_element_type=jnp.float32
    )
    return (jax.nn.sigmoid(gate.astype(jnp.float32)) * total).astype(bf)


def solution(mesh):
    spec = P("col", "row", None)
    return jax.shard_map(
        on_device, mesh=mesh, in_specs=(spec, spec, P("col", None)), out_specs=spec, check_vma=False
    )
```

```python
import functools
import math

import jax
import jax.numpy as jnp
import numpy as np
from jax import lax
from jax.experimental import pallas as pl
from jax.experimental.pallas import tpu as pltpu
from jax.sharding import PartitionSpec as P


GROUP = 256
CHUNKS = 2
MIB = 1 << 20


def split_halves(table):
    head = table.astype(jnp.bfloat16)
    return head, (table - head.astype(np.float64)).astype(jnp.bfloat16)


def feature_table(pairs):
    chunks = GROUP // (2 * pairs)
    out = np.zeros((chunks, 2 * pairs, GROUP))
    m = np.arange(GROUP)
    for t in range(chunks):
        for j in range(pairs):
            c = pairs * t + j
            out[t, j] = np.cos(2 * math.pi * (m * c % GROUP) / GROUP)
            out[t, pairs + j] = -np.sin(2 * math.pi * (m * c % GROUP) / GROUP)
        if t == 0:
            out[0, pairs] = np.where(m % 2 == 0, 1.0, -1.0)
    return out


def position_table(inner, scale):
    angle = 2 * math.pi * (np.outer(np.arange(inner), np.arange(inner)) % inner) / inner
    return np.concatenate([np.cos(angle), np.sin(angle)], axis=1) * scale


def twist_table(rows, inner):
    length = rows * inner
    n2 = np.arange(inner)[:, None]
    res = []
    for core in range(2):
        k1 = 2 * np.arange(rows // 2)[None, :] + core
        angle = 2 * math.pi * (n2 * k1 % length) / length
        res.append(np.concatenate([np.cos(angle), np.sin(angle)], axis=1))
    return np.stack(res).astype(np.float32)


def vmem_call(body, outs, scratch, flops, moved, limit=24):
    return pl.pallas_call(
        body,
        out_shape=outs,
        scratch_shapes=scratch,
        compiler_params=pltpu.CompilerParams(vmem_limit_bytes=limit * MIB),
        cost_estimate=pl.CostEstimate(flops=flops, bytes_accessed=moved, transcendentals=0),
    )


def pick_kernel(chips, fast, *refs):
    x_ref, w_ref, narrow_ref = refs[:3]
    outs = [refs[3 + q * chips : 3 + (q + 1) * chips] for q in range(CHUNKS)]
    narrow, *halves = refs[3 + CHUNKS * chips : -3]
    tokens, x_sems, w_sems = refs[-3:]
    row = lax.axis_index("row")
    core, chip = row % 2, row // 2
    lanes = outs[0][0].shape[1]
    pairs = lanes // 2
    chips_per_group = GROUP // (CHUNKS * lanes)
    loads = []
    for zs in range(chips):
        group = (chip ^ zs) // chips_per_group
        columns = pl.ds(pl.multiple_of(group * GROUP, GROUP), GROUP)
        loads.append(pltpu.make_async_copy(x_ref.at[:, columns], tokens.at[zs], x_sems.at[zs]))
    order = [*send_order(chips), 0]
    for zs in order:
        loads[zs].start()
    fetches = [pltpu.make_async_copy(narrow_ref.at[core], narrow, w_sems.at[2])]
    fetches[0].start()
    if fast:
        half = GROUP // 2
        for i, h in enumerate((core, 1 - core)):
            part = w_ref.at[pl.ds(pl.multiple_of(h * half, half), half), :]
            fetches.append(pltpu.make_async_copy(part, halves[i], w_sems.at[i]))
            fetches[-1].start()
    src = lax.broadcasted_iota(jnp.int32, (GROUP, CHUNKS * lanes), 0)
    column = lax.broadcasted_iota(jnp.int32, (GROUP, CHUNKS * lanes), 1)
    lane, j = column % lanes, column % lanes - pairs
    choose = None
    for zs in order:
        if choose is None or chips_per_group > 1:
            part = ((chip ^ zs) % chips_per_group) * CHUNKS + column // lanes
            mirrored = jnp.where((j == 0) & (part == 0), GROUP // 2, GROUP - pairs * part - j)
            wanted = jnp.where(lane < pairs, pairs * part + lane, mirrored)
            choose = (src == wanted).astype(jnp.bfloat16)
        loads[zs].wait()
        got = jnp.dot(tokens[zs], choose, preferred_element_type=jnp.float32).astype(jnp.bfloat16)
        for q in range(CHUNKS):
            outs[q][zs][...] = got[:, q * lanes : (q + 1) * lanes]
    for fetch in fetches:
        fetch.wait()


def twist_kernel(narrow, out):
    for i in range(out.shape[0]):
        out[i] = jnp.broadcast_to(narrow[:, i : i + 1], out.shape[1:])


def stack_kernel(*refs):
    for zs, piece in enumerate(refs[:-1]):
        refs[-1][zs] = piece[...]


def complex_dft(values):
    n = len(values)
    if n == 1:
        return values
    even, odd = complex_dft(values[0::2]), complex_dft(values[1::2])
    low, high = [], []
    for k in range(n // 2):
        c, s = math.cos(2 * math.pi * k / n), math.sin(2 * math.pi * k / n)
        re, im = odd[k]
        if k == 0:
            tr, ti = re, im
        elif 4 * k == n:
            tr, ti = im, -re
        else:
            tr, ti = re * c + im * s, im * c - re * s
        er, ei = even[k]
        low.append((er + tr, ei + ti))
        high.append((er - tr, ei - ti))
    return low + high


def position_kernel(rows, q, *refs):
    chips = rows // 2
    mine, theirs = refs[:chips], refs[chips]
    table_hi, table_lo, twist = refs[chips + 1 : chips + 4]
    *outs, folded, turned_z, spect = refs[chips + 4 :]
    inner, lanes = mine[0].shape
    pairs = lanes // 2
    row = lax.axis_index("row")
    core, chip = row % 2, row // 2
    half = rows // 2

    odd_core = core == 1
    sign = jnp.where(odd_core, -1.0, 1.0).astype(jnp.float32)
    upper = row >= half
    near, far = jnp.where(upper, sign, 1.0), jnp.where(upper, 1.0, sign)

    lane = lax.broadcasted_iota(jnp.int32, (2 * lanes, lanes), 1)
    line = lax.broadcasted_iota(jnp.int32, (2 * lanes, lanes), 0)
    chips_per_group = GROUP // (CHUNKS * lanes)
    first = (chip % chips_per_group == 0) if q == 0 else False
    lone_high = (lane == pairs) & first
    alone = ((lane == 0) | (lane == pairs)) & first
    own = jnp.where((lane < pairs) | lone_high, 1.0, -1.0)
    other = jnp.where(alone, 0.0, 1.0)
    side = jnp.where(line < lanes, near, far)
    there = line % lanes
    entry = jnp.where(there == lane, own, jnp.where(there == (lane + pairs) % lanes, other, 0.0))
    fold = (entry * side).astype(jnp.bfloat16)

    def block(s):
        return mine[s // 2][...] if s % 2 == 0 else theirs[s // 2]

    for s in range(half):
        both = jnp.concatenate([block(s), block(s ^ half)], axis=1)
        folded[(row % half) ^ s] = jnp.dot(both, fold, preferred_element_type=jnp.float32)

    lane = lax.broadcasted_iota(jnp.int32, (1, lanes), 1)
    cosine = (lane < pairs) | ((lane == pairs) & first)
    turns = []
    for n in range(half):
        angle = 2 * math.pi * n / rows
        c = jnp.where(odd_core, math.cos(angle), 1.0).astype(jnp.float32)
        d = jnp.where(odd_core, math.sin(angle), 0.0).astype(jnp.float32)
        turns.append((jnp.where(cosine, c, d), jnp.where(cosine, -d, c)))
    tile = min(inner, 128)

    def step(i, carry):
        at = pl.ds(pl.multiple_of(i * tile, tile), tile)
        low_at = pl.ds(pl.multiple_of(inner + i * tile, tile), tile)
        values = []
        for n in range(half):
            v = folded[n, at, :]
            values.append((v * turns[n][0], v * turns[n][1]))
        for j, (a, b) in enumerate(complex_dft(values)):
            c, s = twist[j, at, :], twist[half + j, at, :]
            cols = slice(j * lanes, (j + 1) * lanes)
            turned_z[at, cols] = (a * c + b * s).astype(jnp.bfloat16)
            turned_z[low_at, cols] = (b * c - a * s).astype(jnp.bfloat16)
        return carry

    lax.fori_loop(0, inner // tile, step, 0)
    width = min(half * lanes, 256)
    for start in range(0, half * lanes, width):
        cols = slice(start, start + width)
        value = jnp.dot(table_hi[...], turned_z[:, cols], preferred_element_type=jnp.float32)
        value += jnp.dot(table_lo[...], turned_z[:, cols], preferred_element_type=jnp.float32)
        for j in range(start // lanes, (start + width) // lanes):
            piece = value[:, j * lanes - start : (j + 1) * lanes - start]
            spect[j] = piece
    per = inner // rows
    for zs in range(chips):
        for rel in range(2):
            dest = row ^ (2 * zs + rel)
            for j in range(half):
                piece = spect[j, pl.ds(pl.multiple_of(dest * per, per), per), :]
                lines = slice(j * per, (j + 1) * per)
                if q == 0:
                    outs[zs][rel, lines, :] = piece.astype(jnp.bfloat16)
                else:
                    outs[rel][zs, lines, :] = piece.astype(jnp.bfloat16)


def order_rows(rows, count):
    core = lax.axis_index("row") % 2
    half, per = rows // 2, count // rows
    natural = lax.broadcasted_iota(jnp.int32, (count, count), 0)
    received = lax.broadcasted_iota(jnp.int32, (count, count), 1)
    rel, j, k2 = received // (half * per), received // per % half, received % per
    return (natural == rows * k2 + 2 * j + (core ^ rel)).astype(jnp.bfloat16)


def give_kernel(*refs):
    out = refs[-1]
    for zs, ref in enumerate(refs[:-1]):
        out[zs] = ref[1]


def join_kernel(keep, got, *outs):
    for zs, out in enumerate(outs):
        out[0] = keep[zs]
        out[1] = got[zs]


def channel_part(order, pieces, feat_hi, feat_lo):
    lanes = feat_hi.shape[0]
    got = jnp.concatenate([jnp.concatenate(piece, axis=0) for piece in pieces], axis=1)
    got = jnp.dot(order, got, preferred_element_type=jnp.float32).astype(jnp.bfloat16)
    parts = []
    for zs in range(len(pieces)):
        piece = got[:, zs * lanes : (zs + 1) * lanes]
        part = jnp.dot(piece, feat_hi, preferred_element_type=jnp.float32)
        parts.append(part + jnp.dot(piece, feat_lo, preferred_element_type=jnp.float32))
    return parts


def prepare_kernel(rows, *refs):
    chips = rows // 2
    mine, theirs, feat_hi, feat_lo, gate_ref = refs[:chips], *refs[chips : chips + 4]
    spect, opened = refs[chips + 4 :]
    order = order_rows(rows, gate_ref.shape[0])
    pieces = [(ref[0], theirs[zs]) for zs, ref in enumerate(mine)]
    for zs, part in enumerate(channel_part(order, pieces, feat_hi[...], feat_lo[...])):
        spect[zs] = part
    for start in range(0, gate_ref.shape[1], GROUP):
        cols = slice(start, start + GROUP)
        opened[:, cols] = jax.nn.sigmoid(gate_ref[:, cols].astype(jnp.float32))


def final_kernel(rows, *refs):
    chips = rows // 2
    mine, feat_hi, feat_lo, spect, opened = refs[:chips], *refs[chips : chips + 4]
    w_mine, w_rest, w_a, w_b, w_c, v_a, v_b, v_c, out_ref, lhs, result, sems = refs[chips + 4 :]
    count, width = opened.shape
    half = GROUP // 2
    row, col = lax.axis_index("row"), lax.axis_index("col")
    core, chip = row % 2, row // 2
    order = order_rows(rows, count)
    pieces = [(ref[0], ref[1]) for ref in mine]
    for zs, part in enumerate(channel_part(order, pieces, feat_hi[...], feat_lo[...])):
        whole = (part + spect[zs]).astype(jnp.bfloat16)
        for h in range(2):
            spot = pl.ds(pl.multiple_of((core ^ h) * half, half), half)
            lhs[zs, :, spot] = whole[:, h * half : (h + 1) * half]
    weights = (
        (0, w_mine, w_rest),
        (1 + core, w_a, v_b),
        (2 - core, w_b, v_a),
        (3, w_c, v_c),
    )
    copies = []
    for t in range(width // GROUP):
        cols = slice(t * GROUP, (t + 1) * GROUP)
        total = jnp.zeros((count, GROUP), jnp.float32)
        for s, w_here, w_there in weights:
            rhs = jnp.concatenate([w_here[:, cols], w_there[:, cols]], axis=0)
            total += jnp.dot(lhs[chip ^ col ^ s], rhs, preferred_element_type=jnp.float32)
        result[:, cols] = (opened[:, cols] * total).astype(jnp.bfloat16)
        copies.append(pltpu.make_async_copy(result.at[:, cols], out_ref.at[:, cols], sems.at[t]))
        copies[-1].start()
    for copy in copies:
        copy.wait()


def swap(value, axis, size, bit):
    return lax.ppermute(value, axis, [(i, i ^ bit) for i in range(size)])


def turn_swap(value, rows, n_col, bits):
    turn = [
        (row * n_col + col, row * n_col + (col ^ bits[row % 2]))
        for row in range(rows)
        for col in range(n_col)
    ]
    return lax.ppermute(value, ("row", "col"), turn)


def send_order(chips):
    return sorted(range(1, chips), key=lambda zs: (zs < 2, zs))


def across_chips(pieces, rows):
    chips = rows // 2
    got = [pieces[0]] + [None] * (chips - 1)
    for zs in send_order(chips):
        got[zs] = swap(pieces[zs], "row", rows, 2 * zs)
    return got


def on_device(mix_input, gate_logits, w_proj):
    return program(mix_input[0], gate_logits[0], w_proj)[None]


def program(tokens, gate, w_proj):
    count, features = tokens.shape
    rows, n_col = lax.axis_size("row"), lax.axis_size("col")
    chips = rows // 2
    lanes = features // (chips * CHUNKS)
    half = rows // 2
    width = w_proj.shape[1]
    scale = 1.0 / math.sqrt(count * rows * GROUP)
    table_hi, table_lo = split_halves(position_table(count, scale))
    narrow = jnp.asarray(twist_table(rows, count))
    features_of = feature_table(lanes // 2)
    feat_hi, feat_lo = split_halves(features_of)
    bf = jnp.bfloat16
    fast = w_proj.shape[0] == GROUP and CHUNKS * lanes == GROUP and n_col == chips == 4

    half_w = jax.ShapeDtypeStruct((GROUP // 2, width), bf)
    picked = pl.pallas_call(
        functools.partial(pick_kernel, chips, fast),
        out_shape=[jax.ShapeDtypeStruct((count, lanes), bf)] * (CHUNKS * chips)
        + [jax.ShapeDtypeStruct((count, rows), jnp.float32)]
        + [half_w] * (2 * fast),
        in_specs=[pl.BlockSpec(memory_space=pltpu.HBM)] * 3,
        out_specs=[pl.BlockSpec(memory_space=pltpu.VMEM)] * (CHUNKS * chips + 1 + 2 * fast),
        scratch_shapes=[
            pltpu.VMEM((chips, count, GROUP), bf),
            pltpu.SemaphoreType.DMA((chips,)),
            pltpu.SemaphoreType.DMA((3,)),
        ],
        compiler_params=pltpu.CompilerParams(vmem_limit_bytes=24 * MIB),
        cost_estimate=pl.CostEstimate(
            flops=2 * count * GROUP * features, bytes_accessed=MIB, transcendentals=0
        ),
    )(*(pltpu.with_memory_space_constraint(v, pltpu.HBM) for v in (tokens, w_proj, narrow)))
    arrived = [across_chips(picked[q * chips : (q + 1) * chips], rows) for q in range(CHUNKS)]

    if fast:
        mine, rest = picked[CHUNKS * chips + 1 :]
        w_a = turn_swap(mine, rows, n_col, (1, 2))
        w_b = turn_swap(mine, rows, n_col, (2, 1))
        w_c = turn_swap(w_a, rows, n_col, (2, 1))
        others = []
        for own in (w_a, w_b, w_c):
            others.append(swap(own, "row", rows, 1))

    lines = half * (count // rows)
    piece = jax.ShapeDtypeStruct((2, lines, lanes), bf)
    small = (count * features // 4, count * features)
    stacked = jax.ShapeDtypeStruct((chips, lines, lanes), bf)
    twist = vmem_call(
        twist_kernel, jax.ShapeDtypeStruct((rows, count, lanes), jnp.float32), [], *small
    )(picked[CHUNKS * chips])
    sent = []
    for q in range(CHUNKS):
        stack = vmem_call(
            stack_kernel, jax.ShapeDtypeStruct((chips, count, lanes), bf), [], *small
        )(*arrived[q])
        theirs = swap(stack, "row", rows, 1)
        sent.append(
            vmem_call(
                functools.partial(position_kernel, rows, q),
                [piece] * chips if q == 0 else [stacked] * 2,
                [
                    pltpu.VMEM((half, count, lanes), jnp.float32),
                    pltpu.VMEM((2 * count, half * lanes), bf),
                    pltpu.VMEM((half, count, lanes), jnp.float32),
                ],
                8 * count * count * half * lanes,
                rows * count * lanes * 4,
            )(*arrived[q], theirs, table_hi, table_lo, twist)
        )
    early = across_chips(sent[0], rows)
    give = vmem_call(give_kernel, stacked, [], *small)(*early)
    early.append(swap(give, "row", rows, 1))
    keep, give = sent[1]
    got = swap(give, "row", rows, 1)
    joined = vmem_call(join_kernel, [piece] * chips, [], *small)(keep, got)
    late = across_chips(joined, rows)
    if fast:
        spect, opened = vmem_call(
            functools.partial(prepare_kernel, rows),
            [
                jax.ShapeDtypeStruct((chips, count, GROUP), jnp.float32),
                jax.ShapeDtypeStruct((count, width), jnp.float32),
            ],
            [],
            2 * count * features * GROUP,
            6 * count * width,
        )(*early, feat_hi[0], feat_lo[0], gate)
        return pl.pallas_call(
            functools.partial(final_kernel, rows),
            out_shape=jax.ShapeDtypeStruct((count, width), bf),
            in_specs=[pl.BlockSpec(memory_space=pltpu.VMEM)] * (chips + 12),
            out_specs=pl.BlockSpec(memory_space=pl.ANY),
            scratch_shapes=[
                pltpu.VMEM((chips, count, GROUP), bf),
                pltpu.VMEM((count, width), bf),
                pltpu.SemaphoreType.DMA((width // GROUP,)),
            ],
            compiler_params=pltpu.CompilerParams(vmem_limit_bytes=32 * MIB),
            cost_estimate=pl.CostEstimate(
                flops=2 * count * features * width,
                bytes_accessed=2 * features * width,
                transcendentals=0,
            ),
        )(*late, feat_hi[1], feat_lo[1], spect, opened, mine, rest, w_a, w_b, w_c, *others)

    weights = lax.all_gather(w_proj, "col", axis=0, tiled=True).reshape(-1, GROUP, width)
    order = order_rows(rows, count)
    chip = lax.axis_index("row") // 2
    table = jnp.asarray(features_of, jnp.float32).reshape(-1, CHUNKS, lanes, GROUP)
    per_group = table.shape[0]
    spectrum = jnp.zeros((count, weights.shape[0], GROUP), jnp.float32)
    here = chip ^ jnp.arange(chips)
    for q in range(CHUNKS):
        if q == 0:
            parts = [(early[zs][0], early[chips][zs]) for zs in range(chips)]
        else:
            parts = [(ref[0], ref[1]) for ref in late]
        got = jnp.stack([jnp.concatenate(pair, axis=0) for pair in parts])[here]
        got = jnp.einsum("kr,zrl->kzl", order, got, preferred_element_type=jnp.float32)
        spectrum += jnp.einsum(
            "kgtl,tlm->kgm",
            got.reshape(count, -1, per_group, lanes),
            table[:, q],
            precision=lax.Precision.HIGHEST,
        )
    total = jnp.einsum(
        "kgm,gmd->kd", spectrum.astype(bf), weights, preferred_element_type=jnp.float32
    )
    return (jax.nn.sigmoid(gate.astype(jnp.float32)) * total).astype(bf)


def solution(mesh):
    spec = P("col", "row", None)
    return jax.shard_map(
        on_device, mesh=mesh, in_specs=(spec, spec, P("col", None)), out_specs=spec, check_vma=False
    )
```

```python
import functools
import math

import jax
import jax.numpy as jnp
import numpy as np
from jax import lax
from jax.experimental import pallas as pl
from jax.experimental.pallas import tpu as pltpu
from jax.sharding import PartitionSpec as P


GROUP = 256
CHUNKS = 2
NEAR = 1
MIB = 1 << 20


def split_halves(table):
    head = table.astype(jnp.bfloat16)
    return head, (table - head.astype(np.float64)).astype(jnp.bfloat16)


def feature_table(pairs):
    chunks = GROUP // (2 * pairs)
    out = np.zeros((chunks, 2 * pairs, GROUP))
    m = np.arange(GROUP)
    for t in range(chunks):
        for j in range(pairs):
            c = pairs * t + j
            out[t, j] = np.cos(2 * math.pi * (m * c % GROUP) / GROUP)
            out[t, pairs + j] = -np.sin(2 * math.pi * (m * c % GROUP) / GROUP)
        if t == 0:
            out[0, pairs] = np.where(m % 2 == 0, 1.0, -1.0)
    return out


def position_table(inner, scale):
    angle = 2 * math.pi * (np.outer(np.arange(inner), np.arange(inner)) % inner) / inner
    return np.concatenate([np.cos(angle), np.sin(angle)], axis=1) * scale


def twist_table(rows, inner):
    length = rows * inner
    n2 = np.arange(inner)[:, None]
    res = []
    for core in range(2):
        k1 = 2 * np.arange(rows // 2)[None, :] + core
        angle = 2 * math.pi * (n2 * k1 % length) / length
        res.append(np.concatenate([np.cos(angle), np.sin(angle)], axis=1))
    return np.stack(res).astype(np.float32)


def vmem_call(body, outs, scratch, flops, moved, limit=24):
    return pl.pallas_call(
        body,
        out_shape=outs,
        scratch_shapes=scratch,
        compiler_params=pltpu.CompilerParams(vmem_limit_bytes=limit * MIB),
        cost_estimate=pl.CostEstimate(flops=flops, bytes_accessed=moved, transcendentals=0),
    )


def pick_kernel(chips, fast, *refs):
    x_ref, w_ref, narrow_ref = refs[:3]
    outs = refs[3 : 3 + CHUNKS * chips - 1]
    narrow, *halves = refs[2 + CHUNKS * chips : -3]
    tokens, x_sems, w_sems = refs[-3:]
    row = lax.axis_index("row")
    core, chip = row % 2, row // 2
    lanes = outs[0].shape[1]
    pairs = lanes // 2
    chips_per_group = GROUP // (CHUNKS * lanes)
    loads = []
    for zs in range(chips):
        group = (chip ^ zs) // chips_per_group
        columns = pl.ds(pl.multiple_of(group * GROUP, GROUP), GROUP)
        loads.append(pltpu.make_async_copy(x_ref.at[:, columns], tokens.at[zs], x_sems.at[zs]))
    order = [*send_order(chips), 0]
    for zs in order:
        loads[zs].start()
    fetches = [pltpu.make_async_copy(narrow_ref.at[core], narrow, w_sems.at[2])]
    fetches[0].start()
    if fast:
        half = GROUP // 2
        for i, h in enumerate((core, 1 - core)):
            part = w_ref.at[pl.ds(pl.multiple_of(h * half, half), half), :]
            fetches.append(pltpu.make_async_copy(part, halves[i], w_sems.at[i]))
            fetches[-1].start()
    src = lax.broadcasted_iota(jnp.int32, (GROUP, CHUNKS * lanes), 0)
    column = lax.broadcasted_iota(jnp.int32, (GROUP, CHUNKS * lanes), 1)
    lane, j = column % lanes, column % lanes - pairs
    choose = None
    for zs in order:
        if choose is None or chips_per_group > 1:
            part = ((chip ^ zs) % chips_per_group) * CHUNKS + column // lanes
            mirrored = jnp.where((j == 0) & (part == 0), GROUP // 2, GROUP - pairs * part - j)
            wanted = jnp.where(lane < pairs, pairs * part + lane, mirrored)
            choose = (src == wanted).astype(jnp.bfloat16)
        loads[zs].wait()
        got = jnp.dot(tokens[zs], choose, preferred_element_type=jnp.float32).astype(jnp.bfloat16)
        for q in range(CHUNKS):
            piece = got[:, q * lanes : (q + 1) * lanes]
            if zs == NEAR:
                outs[NEAR][q] = piece
            else:
                outs[zs + q * (chips - (zs > NEAR))][...] = piece
    for fetch in fetches:
        fetch.wait()


def twist_kernel(narrow, out):
    for i in range(out.shape[0]):
        out[i] = jnp.broadcast_to(narrow[:, i : i + 1], out.shape[1:])


def stack_kernel(q, *refs):
    for zs, piece in enumerate(refs[:-1]):
        refs[-1][zs] = piece[q] if zs == NEAR else piece[...]


def complex_dft(values):
    n = len(values)
    if n == 1:
        return values
    even, odd = complex_dft(values[0::2]), complex_dft(values[1::2])
    low, high = [], []
    for k in range(n // 2):
        c, s = math.cos(2 * math.pi * k / n), math.sin(2 * math.pi * k / n)
        re, im = odd[k]
        if k == 0:
            tr, ti = re, im
        elif 4 * k == n:
            tr, ti = im, -re
        else:
            tr, ti = re * c + im * s, im * c - re * s
        er, ei = even[k]
        low.append((er + tr, ei + ti))
        high.append((er - tr, ei - ti))
    return low + high


def position_kernel(rows, q, *refs):
    chips = rows // 2
    mine, theirs = refs[:chips], refs[chips]
    table_hi, table_lo, twist = refs[chips + 1 : chips + 4]
    *outs, folded, turned_z, spect = refs[chips + 4 :]
    if q == 1:
        near_give, *outs = outs
        outs[1][chips] = near_give[...]
    inner, lanes = mine[0].shape
    pairs = lanes // 2
    row = lax.axis_index("row")
    core, chip = row % 2, row // 2
    half = rows // 2

    odd_core = core == 1
    sign = jnp.where(odd_core, -1.0, 1.0).astype(jnp.float32)
    upper = row >= half
    here, away = jnp.where(upper, sign, 1.0), jnp.where(upper, 1.0, sign)

    lane = lax.broadcasted_iota(jnp.int32, (2 * lanes, lanes), 1)
    line = lax.broadcasted_iota(jnp.int32, (2 * lanes, lanes), 0)
    chips_per_group = GROUP // (CHUNKS * lanes)
    first = (chip % chips_per_group == 0) if q == 0 else False
    lone_high = (lane == pairs) & first
    alone = ((lane == 0) | (lane == pairs)) & first
    own = jnp.where((lane < pairs) | lone_high, 1.0, -1.0)
    other = jnp.where(alone, 0.0, 1.0)
    side = jnp.where(line < lanes, here, away)
    there = line % lanes
    entry = jnp.where(there == lane, own, jnp.where(there == (lane + pairs) % lanes, other, 0.0))
    fold = (entry * side).astype(jnp.bfloat16)

    def block(s):
        if s % 2 == 1:
            return theirs[s // 2]
        return mine[NEAR][q] if s // 2 == NEAR else mine[s // 2][...]

    for s in range(half):
        both = jnp.concatenate([block(s), block(s ^ half)], axis=1)
        folded[(row % half) ^ s] = jnp.dot(both, fold, preferred_element_type=jnp.float32)

    lane = lax.broadcasted_iota(jnp.int32, (1, lanes), 1)
    cosine = (lane < pairs) | ((lane == pairs) & first)
    turns = []
    for n in range(half):
        angle = 2 * math.pi * n / rows
        c = jnp.where(odd_core, math.cos(angle), 1.0).astype(jnp.float32)
        d = jnp.where(odd_core, math.sin(angle), 0.0).astype(jnp.float32)
        turns.append((jnp.where(cosine, c, d), jnp.where(cosine, -d, c)))
    tile = min(inner, 128)

    def step(i, carry):
        at = pl.ds(pl.multiple_of(i * tile, tile), tile)
        low_at = pl.ds(pl.multiple_of(inner + i * tile, tile), tile)
        values = []
        for n in range(half):
            v = folded[n, at, :]
            values.append((v * turns[n][0], v * turns[n][1]))
        for j, (a, b) in enumerate(complex_dft(values)):
            c, s = twist[j, at, :], twist[half + j, at, :]
            cols = slice(j * lanes, (j + 1) * lanes)
            turned_z[at, cols] = (a * c + b * s).astype(jnp.bfloat16)
            turned_z[low_at, cols] = (b * c - a * s).astype(jnp.bfloat16)
        return carry

    lax.fori_loop(0, inner // tile, step, 0)
    width = min(half * lanes, 256)
    for start in range(0, half * lanes, width):
        cols = slice(start, start + width)
        value = jnp.dot(table_hi[...], turned_z[:, cols], preferred_element_type=jnp.float32)
        value += jnp.dot(table_lo[...], turned_z[:, cols], preferred_element_type=jnp.float32)
        for j in range(start // lanes, (start + width) // lanes):
            piece = value[:, j * lanes - start : (j + 1) * lanes - start]
            spect[j] = piece
    per = inner // rows
    for zs in range(chips):
        for rel in range(2):
            dest = row ^ (2 * zs + rel)
            for j in range(half):
                piece = spect[j, pl.ds(pl.multiple_of(dest * per, per), per), :]
                lines = slice(j * per, (j + 1) * per)
                if q == 1:
                    outs[rel][zs, lines, :] = piece.astype(jnp.bfloat16)
                elif zs == NEAR:
                    outs[chips - 1 + rel][lines, :] = piece.astype(jnp.bfloat16)
                else:
                    outs[zs - (zs > NEAR)][rel, lines, :] = piece.astype(jnp.bfloat16)


def order_rows(rows, count):
    core = lax.axis_index("row") % 2
    half, per = rows // 2, count // rows
    natural = lax.broadcasted_iota(jnp.int32, (count, count), 0)
    received = lax.broadcasted_iota(jnp.int32, (count, count), 1)
    rel, j, k2 = received // (half * per), received // per % half, received % per
    return (natural == rows * k2 + 2 * j + (core ^ rel)).astype(jnp.bfloat16)


def give_kernel(*refs):
    out = refs[-1]
    for zs, ref in enumerate(refs[:-1]):
        out[zs] = ref[1]


def join_kernel(keep, got, near_keep, *outs):
    for zs, out in enumerate(outs):
        out[0] = keep[zs]
        out[1] = got[zs]
    outs[NEAR][2] = near_keep[...]
    outs[NEAR][3] = got[len(outs)]


def in_order(order, pieces):
    lanes = pieces[0][0].shape[1]
    got = jnp.concatenate([jnp.concatenate(piece, axis=0) for piece in pieces], axis=1)
    got = jnp.dot(order, got, preferred_element_type=jnp.float32).astype(jnp.bfloat16)
    return [got[:, i * lanes : (i + 1) * lanes] for i in range(len(pieces))]


def channel_part(piece, feat_hi, feat_lo):
    part = jnp.dot(piece, feat_hi, preferred_element_type=jnp.float32)
    return part + jnp.dot(piece, feat_lo, preferred_element_type=jnp.float32)


def all_but_near(chips):
    return [zs for zs in range(chips) if zs != NEAR]


def prepare_kernel(rows, *refs):
    chips = rows // 2
    far = all_but_near(chips)
    mine, theirs, feat_hi, feat_lo, gate_ref = refs[: chips - 1], *refs[chips - 1 : chips + 3]
    spect, opened = refs[chips + 3 :]
    order = order_rows(rows, gate_ref.shape[0])
    pieces = [(ref[0], theirs[i]) for i, ref in enumerate(mine)]
    for zs, piece in zip(far, in_order(order, pieces)):
        spect[zs] = channel_part(piece, feat_hi[...], feat_lo[...])
    for start in range(0, gate_ref.shape[1], GROUP):
        cols = slice(start, start + GROUP)
        opened[:, cols] = jax.nn.sigmoid(gate_ref[:, cols].astype(jnp.float32))


def final_kernel(rows, *refs):
    chips = rows // 2
    mine, feat_hi, feat_lo, spect, opened = refs[:chips], *refs[chips : chips + 4]
    w_mine, w_rest, w_a, w_b, w_c, v_a, v_b, v_c, out_ref, lhs, result, sems = refs[chips + 4 :]
    count, width = opened.shape
    half = GROUP // 2
    row, col = lax.axis_index("row"), lax.axis_index("col")
    core, chip = row % 2, row // 2
    order = order_rows(rows, count)
    pieces = [(ref[0], ref[1]) for ref in mine] + [(mine[NEAR][2], mine[NEAR][3])]
    *late, near_early = in_order(order, pieces)
    for zs, piece in enumerate(late):
        if zs == NEAR:
            early = channel_part(near_early, feat_hi[0], feat_lo[0])
        else:
            early = spect[zs]
        whole = (channel_part(piece, feat_hi[1], feat_lo[1]) + early).astype(jnp.bfloat16)
        for h in range(2):
            spot = pl.ds(pl.multiple_of((core ^ h) * half, half), half)
            lhs[zs, :, spot] = whole[:, h * half : (h + 1) * half]
    weights = (
        (0, w_mine, w_rest),
        (1 + core, w_a, v_b),
        (2 - core, w_b, v_a),
        (3, w_c, v_c),
    )
    copies = []
    for t in range(width // GROUP):
        cols = slice(t * GROUP, (t + 1) * GROUP)
        total = jnp.zeros((count, GROUP), jnp.float32)
        for s, w_here, w_there in weights:
            rhs = jnp.concatenate([w_here[:, cols], w_there[:, cols]], axis=0)
            total += jnp.dot(lhs[chip ^ col ^ s], rhs, preferred_element_type=jnp.float32)
        result[:, cols] = (opened[:, cols] * total).astype(jnp.bfloat16)
        copies.append(pltpu.make_async_copy(result.at[:, cols], out_ref.at[:, cols], sems.at[t]))
        copies[-1].start()
    for copy in copies:
        copy.wait()


def swap(value, axis, size, bit):
    return lax.ppermute(value, axis, [(i, i ^ bit) for i in range(size)])


def turn_swap(value, rows, n_col, bits):
    turn = [
        (row * n_col + col, row * n_col + (col ^ bits[row % 2]))
        for row in range(rows)
        for col in range(n_col)
    ]
    return lax.ppermute(value, ("row", "col"), turn)


def send_order(chips):
    return sorted(range(1, chips), key=lambda zs: (zs < 2, zs))


def across_chips(pieces, rows):
    got = dict(pieces)
    for zs in send_order(rows // 2):
        if zs in pieces and zs != NEAR:
            got[zs] = swap(pieces[zs], "row", rows, 2 * zs)
    if NEAR in pieces:
        got[NEAR] = swap(pieces[NEAR], "row", rows, 2 * NEAR)
    return got


def on_device(mix_input, gate_logits, w_proj):
    return program(mix_input[0], gate_logits[0], w_proj)[None]


def program(tokens, gate, w_proj):
    count, features = tokens.shape
    rows, n_col = lax.axis_size("row"), lax.axis_size("col")
    chips = rows // 2
    lanes = features // (chips * CHUNKS)
    half = rows // 2
    width = w_proj.shape[1]
    scale = 1.0 / math.sqrt(count * rows * GROUP)
    table_hi, table_lo = split_halves(position_table(count, scale))
    narrow = jnp.asarray(twist_table(rows, count))
    features_of = feature_table(lanes // 2)
    feat_hi, feat_lo = split_halves(features_of)
    bf = jnp.bfloat16
    fast = w_proj.shape[0] == GROUP and CHUNKS * lanes == GROUP and n_col == chips == 4

    half_w = jax.ShapeDtypeStruct((GROUP // 2, width), bf)
    picked = pl.pallas_call(
        functools.partial(pick_kernel, chips, fast),
        out_shape=[jax.ShapeDtypeStruct((count, lanes), bf)]
        + [jax.ShapeDtypeStruct((CHUNKS, count, lanes), bf)]
        + [jax.ShapeDtypeStruct((count, lanes), bf)] * (CHUNKS * (chips - 1) - 1)
        + [jax.ShapeDtypeStruct((count, rows), jnp.float32)]
        + [half_w] * (2 * fast),
        in_specs=[pl.BlockSpec(memory_space=pltpu.HBM)] * 3,
        out_specs=[pl.BlockSpec(memory_space=pltpu.VMEM)] * (CHUNKS * chips + 2 * fast),
        scratch_shapes=[
            pltpu.VMEM((chips, count, GROUP), bf),
            pltpu.SemaphoreType.DMA((chips,)),
            pltpu.SemaphoreType.DMA((3,)),
        ],
        compiler_params=pltpu.CompilerParams(vmem_limit_bytes=24 * MIB),
        cost_estimate=pl.CostEstimate(
            flops=2 * count * GROUP * features, bytes_accessed=MIB, transcendentals=0
        ),
    )(*(pltpu.with_memory_space_constraint(v, pltpu.HBM) for v in (tokens, w_proj, narrow)))
    far = all_but_near(chips)
    first = across_chips(dict(enumerate(picked[:chips])), rows)
    second = across_chips(dict(zip(far, picked[chips:])), rows)
    arrived = [[first[zs] for zs in range(chips)]]
    arrived.append([{**second, NEAR: first[NEAR]}[zs] for zs in range(chips)])
    narrow_own, *halves = picked[2 * chips - 1 :]

    if fast:
        mine, rest = halves
        w_a = turn_swap(mine, rows, n_col, (1, 2))
        w_b = turn_swap(mine, rows, n_col, (2, 1))
        w_c = turn_swap(w_a, rows, n_col, (2, 1))
        others = []
        for own in (w_a, w_b, w_c):
            others.append(swap(own, "row", rows, 1))

    lines = half * (count // rows)
    piece = jax.ShapeDtypeStruct((2, lines, lanes), bf)
    small = (count * features // 4, count * features)

    def stacked(n):
        return jax.ShapeDtypeStruct((n, lines, lanes), bf)

    twist = vmem_call(
        twist_kernel, jax.ShapeDtypeStruct((rows, count, lanes), jnp.float32), [], *small
    )(narrow_own)
    line = jax.ShapeDtypeStruct((lines, lanes), bf)
    made = ([piece] * (chips - 1) + [line] * 2, [stacked(chips), stacked(chips + 1)])
    sent = []
    for q in range(CHUNKS):
        stack = vmem_call(
            functools.partial(stack_kernel, q),
            jax.ShapeDtypeStruct((chips, count, lanes), bf),
            [],
            *small,
        )(*arrived[q])
        theirs = swap(stack, "row", rows, 1)
        sent.append(
            vmem_call(
                functools.partial(position_kernel, rows, q),
                made[q],
                [
                    pltpu.VMEM((half, count, lanes), jnp.float32),
                    pltpu.VMEM((2 * count, half * lanes), bf),
                    pltpu.VMEM((half, count, lanes), jnp.float32),
                ],
                8 * count * count * half * lanes,
                rows * count * lanes * 4,
            )(*arrived[q], theirs, table_hi, table_lo, twist, *(sent[0][chips:] if q else ()))
        )
    early = across_chips(dict(zip(far, sent[0])), rows)
    early = [early[zs] for zs in far]
    give = vmem_call(give_kernel, stacked(chips - 1), [], *small)(*early)
    early.append(swap(give, "row", rows, 1))
    keep, give = sent[1]
    got = swap(give, "row", rows, 1)
    joined = vmem_call(
        join_kernel, [stacked(4 if zs == NEAR else 2) for zs in range(chips)], [], *small
    )(keep, got, sent[0][chips - 1])
    late = across_chips(dict(enumerate(joined)), rows)
    late = [late[zs] for zs in range(chips)]
    if fast:
        spect, opened = vmem_call(
            functools.partial(prepare_kernel, rows),
            [
                jax.ShapeDtypeStruct((chips, count, GROUP), jnp.float32),
                jax.ShapeDtypeStruct((count, width), jnp.float32),
            ],
            [],
            2 * count * features * GROUP,
            6 * count * width,
        )(*early, feat_hi[0], feat_lo[0], gate)
        return pl.pallas_call(
            functools.partial(final_kernel, rows),
            out_shape=jax.ShapeDtypeStruct((count, width), bf),
            in_specs=[pl.BlockSpec(memory_space=pltpu.VMEM)] * (chips + 12),
            out_specs=pl.BlockSpec(memory_space=pl.ANY),
            scratch_shapes=[
                pltpu.VMEM((chips, count, GROUP), bf),
                pltpu.VMEM((count, width), bf),
                pltpu.SemaphoreType.DMA((width // GROUP,)),
            ],
            compiler_params=pltpu.CompilerParams(vmem_limit_bytes=32 * MIB),
            cost_estimate=pl.CostEstimate(
                flops=2 * count * features * width,
                bytes_accessed=2 * features * width,
                transcendentals=0,
            ),
        )(*late, feat_hi, feat_lo, spect, opened, mine, rest, w_a, w_b, w_c, *others)

    weights = lax.all_gather(w_proj, "col", axis=0, tiled=True).reshape(-1, GROUP, width)
    order = order_rows(rows, count)
    chip = lax.axis_index("row") // 2
    table = jnp.asarray(features_of, jnp.float32).reshape(-1, CHUNKS, lanes, GROUP)
    per_group = table.shape[0]
    spectrum = jnp.zeros((count, weights.shape[0], GROUP), jnp.float32)
    here = chip ^ jnp.arange(chips)
    for q in range(CHUNKS):
        if q == 0:
            parts = [(early[i][0], early[-1][i]) for i in range(chips - 1)]
            parts.insert(NEAR, (late[NEAR][2], late[NEAR][3]))
        else:
            parts = [(ref[0], ref[1]) for ref in late]
        got = jnp.stack([jnp.concatenate(pair, axis=0) for pair in parts])[here]
        got = jnp.einsum("kr,zrl->kzl", order, got, preferred_element_type=jnp.float32)
        spectrum += jnp.einsum(
            "kgtl,tlm->kgm",
            got.reshape(count, -1, per_group, lanes),
            table[:, q],
            precision=lax.Precision.HIGHEST,
        )
    total = jnp.einsum(
        "kgm,gmd->kd", spectrum.astype(bf), weights, preferred_element_type=jnp.float32
    )
    return (jax.nn.sigmoid(gate.astype(jnp.float32)) * total).astype(bf)


def solution(mesh):
    spec = P("col", "row", None)
    return jax.shard_map(
        on_device, mesh=mesh, in_specs=(spec, spec, P("col", None)), out_specs=spec, check_vma=False
    )
```

```python
import functools
import math

import jax
import jax.numpy as jnp
import numpy as np
from jax import lax
from jax.experimental import pallas as pl
from jax.experimental.pallas import tpu as pltpu
from jax.sharding import PartitionSpec as P


GROUP = 256
CHUNKS = 2
SPAN = 2
NEAR = 1
MIB = 1 << 20


def split_halves(table):
    head = table.astype(jnp.bfloat16)
    return head, (table - head.astype(np.float64)).astype(jnp.bfloat16)


def feature_table(pairs):
    chunks = GROUP // (2 * pairs)
    out = np.zeros((chunks, 2 * pairs, GROUP))
    m = np.arange(GROUP)
    for t in range(chunks):
        for j in range(pairs):
            c = pairs * t + j
            out[t, j] = np.cos(2 * math.pi * (m * c % GROUP) / GROUP)
            out[t, pairs + j] = -np.sin(2 * math.pi * (m * c % GROUP) / GROUP)
        if t == 0:
            out[0, pairs] = np.where(m % 2 == 0, 1.0, -1.0)
    return out


def position_table(inner, scale):
    angle = 2 * math.pi * (np.outer(np.arange(inner), np.arange(inner)) % inner) / inner
    return np.concatenate([np.cos(angle), np.sin(angle)], axis=1) * scale


def twist_table(rows, inner):
    length = rows * inner
    n2 = np.arange(inner)[:, None]
    res = []
    for core in range(2):
        k1 = 2 * np.arange(rows // 2)[None, :] + core
        angle = 2 * math.pi * (n2 * k1 % length) / length
        res.append(np.concatenate([np.cos(angle), np.sin(angle)], axis=1))
    return np.stack(res).astype(np.float32)


def vmem_call(body, outs, scratch, flops, moved, limit=24):
    return pl.pallas_call(
        body,
        out_shape=outs,
        scratch_shapes=scratch,
        compiler_params=pltpu.CompilerParams(vmem_limit_bytes=limit * MIB),
        cost_estimate=pl.CostEstimate(flops=flops, bytes_accessed=moved, transcendentals=0),
    )


def pick_kernel(chips, fast, *refs):
    x_ref, w_ref, narrow_ref = refs[:3]
    outs = refs[3 : 3 + CHUNKS * chips - 1]
    narrow, *halves = refs[2 + CHUNKS * chips : -3]
    tokens, x_sem, w_sems = refs[-3:]
    row = lax.axis_index("row")
    core, chip = row % 2, row // 2
    lanes = outs[0].shape[1]
    pairs = lanes // 2
    chips_per_group = GROUP // (CHUNKS * lanes)
    load = pltpu.make_async_copy(x_ref, tokens, x_sem)
    load.start()
    fetches = [pltpu.make_async_copy(narrow_ref.at[core], narrow, w_sems.at[2])]
    fetches[0].start()
    if fast:
        half = GROUP // 2
        for i, h in enumerate((core, 1 - core)):
            part = w_ref.at[pl.ds(pl.multiple_of(h * half, half), half), :]
            fetches.append(pltpu.make_async_copy(part, halves[i], w_sems.at[i]))
            fetches[-1].start()
    src = lax.broadcasted_iota(jnp.int32, (GROUP, CHUNKS * lanes), 0)
    column = lax.broadcasted_iota(jnp.int32, (GROUP, CHUNKS * lanes), 1)
    lane, j = column % lanes, column % lanes - pairs

    def chosen(zs):
        part = ((chip ^ zs) % chips_per_group) * CHUNKS + column // lanes
        mirrored = jnp.where((j == 0) & (part == 0), GROUP // 2, GROUP - pairs * part - j)
        return (src == jnp.where(lane < pairs, pairs * part + lane, mirrored)).astype(jnp.bfloat16)

    same = chosen(0) if chips_per_group == 1 else None
    load.wait()
    for zs in range(chips):
        group = (chip ^ zs) // chips_per_group
        block = tokens[:, pl.ds(pl.multiple_of(group * GROUP, GROUP), GROUP)]
        choose = chosen(zs) if same is None else same
        got = jnp.dot(block, choose, preferred_element_type=jnp.float32).astype(jnp.bfloat16)
        for q in range(CHUNKS):
            piece = got[:, q * lanes : (q + 1) * lanes]
            if zs == NEAR:
                outs[NEAR][q] = piece
            else:
                outs[zs + q * (chips - (zs > NEAR))][...] = piece
    for fetch in fetches:
        fetch.wait()


def twist_kernel(narrow, out):
    for i in range(out.shape[0]):
        out[i] = jnp.broadcast_to(narrow[:, i : i + 1], out.shape[1:])


def stack_kernel(q, *refs):
    for zs, piece in enumerate(refs[:-1]):
        refs[-1][zs] = piece[q] if zs == NEAR else piece[...]


def complex_dft(values):
    n = len(values)
    if n == 1:
        return values
    even, odd = complex_dft(values[0::2]), complex_dft(values[1::2])
    low, high = [], []
    for k in range(n // 2):
        c, s = math.cos(2 * math.pi * k / n), math.sin(2 * math.pi * k / n)
        re, im = odd[k]
        if k == 0:
            tr, ti = re, im
        elif 4 * k == n:
            tr, ti = im, -re
        else:
            tr, ti = re * c + im * s, im * c - re * s
        er, ei = even[k]
        low.append((er + tr, ei + ti))
        high.append((er - tr, ei - ti))
    return low + high


def position_kernel(rows, q, *refs):
    chips = rows // 2
    mine, theirs = refs[:chips], refs[chips]
    table_hi, table_lo, twist = refs[chips + 1 : chips + 4]
    *outs, folded, turned_z, spect = refs[chips + 4 :]
    if q == 1:
        near_give, *outs = outs
        outs[1][chips] = near_give[...]
    inner, lanes = mine[0].shape
    pairs = lanes // 2
    row = lax.axis_index("row")
    core, chip = row % 2, row // 2
    half = rows // 2

    odd_core = core == 1
    sign = jnp.where(odd_core, -1.0, 1.0).astype(jnp.float32)
    upper = row >= half
    here, away = jnp.where(upper, sign, 1.0), jnp.where(upper, 1.0, sign)

    lane = lax.broadcasted_iota(jnp.int32, (2 * lanes, lanes), 1)
    line = lax.broadcasted_iota(jnp.int32, (2 * lanes, lanes), 0)
    chips_per_group = GROUP // (CHUNKS * lanes)
    first = (chip % chips_per_group == 0) if q == 0 else False
    lone_high = (lane == pairs) & first
    alone = ((lane == 0) | (lane == pairs)) & first
    own = jnp.where((lane < pairs) | lone_high, 1.0, -1.0)
    other = jnp.where(alone, 0.0, 1.0)
    side = jnp.where(line < lanes, here, away)
    there = line % lanes
    entry = jnp.where(there == lane, own, jnp.where(there == (lane + pairs) % lanes, other, 0.0))
    fold = (entry * side).astype(jnp.bfloat16)

    def block(s):
        if s % 2 == 1:
            return theirs[s // 2]
        return mine[NEAR][q] if s // 2 == NEAR else mine[s // 2][...]

    for s in range(half):
        both = jnp.concatenate([block(s), block(s ^ half)], axis=1)
        folded[(row % half) ^ s] = jnp.dot(both, fold, preferred_element_type=jnp.float32)

    lane = lax.broadcasted_iota(jnp.int32, (1, lanes), 1)
    cosine = (lane < pairs) | ((lane == pairs) & first)
    turns = []
    for n in range(half):
        angle = 2 * math.pi * n / rows
        c = jnp.where(odd_core, math.cos(angle), 1.0).astype(jnp.float32)
        d = jnp.where(odd_core, math.sin(angle), 0.0).astype(jnp.float32)
        turns.append((jnp.where(cosine, c, d), jnp.where(cosine, -d, c)))
    tile = min(inner, 128)

    def step(i, carry):
        at = pl.ds(pl.multiple_of(i * tile, tile), tile)
        low_at = pl.ds(pl.multiple_of(inner + i * tile, tile), tile)
        values = []
        for n in range(half):
            v = folded[n, at, :]
            values.append((v * turns[n][0], v * turns[n][1]))
        for j, (a, b) in enumerate(complex_dft(values)):
            c, s = twist[j, at, :], twist[half + j, at, :]
            cols = slice(j * lanes, (j + 1) * lanes)
            turned_z[at, cols] = (a * c + b * s).astype(jnp.bfloat16)
            turned_z[low_at, cols] = (b * c - a * s).astype(jnp.bfloat16)
        return carry

    lax.fori_loop(0, inner // tile, step, 0)
    width = min(half * lanes, 256)
    for start in range(0, half * lanes, width):
        cols = slice(start, start + width)
        value = jnp.dot(table_hi[...], turned_z[:, cols], preferred_element_type=jnp.float32)
        value += jnp.dot(table_lo[...], turned_z[:, cols], preferred_element_type=jnp.float32)
        for j in range(start // lanes, (start + width) // lanes):
            piece = value[:, j * lanes - start : (j + 1) * lanes - start]
            spect[j] = piece
    per = inner // rows
    for zs in range(chips):
        for rel in range(2):
            dest = row ^ (2 * zs + rel)
            for j in range(half):
                piece = spect[j, pl.ds(pl.multiple_of(dest * per, per), per), :]
                lines = slice(j * per, (j + 1) * per)
                if q == 1:
                    outs[rel][zs, lines, :] = piece.astype(jnp.bfloat16)
                elif zs == NEAR:
                    outs[chips - 1 + rel][lines, :] = piece.astype(jnp.bfloat16)
                else:
                    outs[zs - (zs > NEAR)][rel, lines, :] = piece.astype(jnp.bfloat16)


def order_rows(rows, count):
    core = lax.axis_index("row") % 2
    half, per = rows // 2, count // rows
    natural = lax.broadcasted_iota(jnp.int32, (count, count), 0)
    received = lax.broadcasted_iota(jnp.int32, (count, count), 1)
    rel, j, k2 = received // (half * per), received // per % half, received % per
    return (natural == rows * k2 + 2 * j + (core ^ rel)).astype(jnp.bfloat16)


def give_kernel(*refs):
    out = refs[-1]
    for zs, ref in enumerate(refs[:-1]):
        out[zs] = ref[1]


def join_kernel(keep, got, near_keep, *outs):
    for zs, out in enumerate(outs):
        out[0] = keep[zs]
        out[1] = got[zs]
    outs[NEAR][2] = near_keep[...]
    outs[NEAR][3] = got[len(outs)]


def in_order(order, pieces):
    lanes = pieces[0][0].shape[1]
    got = jnp.concatenate([jnp.concatenate(piece, axis=0) for piece in pieces], axis=1)
    got = jnp.dot(order, got, preferred_element_type=jnp.float32).astype(jnp.bfloat16)
    return [got[:, i * lanes : (i + 1) * lanes] for i in range(len(pieces))]


def channel_part(piece, feat):
    twice = jnp.concatenate([piece, piece], axis=1)
    return jnp.dot(twice, feat, preferred_element_type=jnp.float32)


def all_but_near(chips):
    return [zs for zs in range(chips) if zs != NEAR]


def prepare_kernel(rows, *refs):
    chips = rows // 2
    far = all_but_near(chips)
    mine, theirs, feat, gate_ref = refs[: chips - 1], *refs[chips - 1 : chips + 2]
    spect, opened = refs[chips + 2 :]
    order = order_rows(rows, gate_ref.shape[0])
    pieces = [(ref[0], theirs[i]) for i, ref in enumerate(mine)]
    for zs, piece in zip(far, in_order(order, pieces)):
        spect[zs] = channel_part(piece, feat[0])
    for start in range(0, gate_ref.shape[1], GROUP):
        cols = slice(start, start + GROUP)
        opened[:, cols] = jax.nn.sigmoid(gate_ref[:, cols].astype(jnp.float32))


def final_kernel(rows, *refs):
    chips = rows // 2
    mine, feat, spect, opened = refs[:chips], *refs[chips : chips + 3]
    w_mine, w_rest, w_a, w_b, w_c, v_a, v_b, v_c, out_ref, lhs, result, sems = refs[chips + 3 :]
    count, width = opened.shape
    half = GROUP // 2
    row, col = lax.axis_index("row"), lax.axis_index("col")
    core, chip = row % 2, row // 2
    order = order_rows(rows, count)
    pieces = [(ref[0], ref[1]) for ref in mine] + [(mine[NEAR][2], mine[NEAR][3])]
    *late, near_early = in_order(order, pieces)
    for zs, piece in enumerate(late):
        if zs == NEAR:
            early = channel_part(near_early, feat[0])
        else:
            early = spect[zs]
        whole = (channel_part(piece, feat[1]) + early).astype(jnp.bfloat16)
        for h in range(2):
            spot = pl.ds(pl.multiple_of((core ^ h) * half, half), half)
            lhs[zs, :, spot] = whole[:, h * half : (h + 1) * half]
    weights = (
        (0, w_mine, w_rest),
        (1 + core, w_a, v_b),
        (2 - core, w_b, v_a),
        (3, w_c, v_c),
    )
    copies = []
    for t in range(width // GROUP):
        cols = slice(t * GROUP, (t + 1) * GROUP)
        total = jnp.zeros((count, GROUP), jnp.float32)
        for s, w_here, w_there in weights:
            rhs = jnp.concatenate([w_here[:, cols], w_there[:, cols]], axis=0)
            total += jnp.dot(lhs[chip ^ col ^ s], rhs, preferred_element_type=jnp.float32)
        result[:, cols] = (opened[:, cols] * total).astype(jnp.bfloat16)
        if (t + 1) % SPAN == 0:
            span = slice((t + 1 - SPAN) * GROUP, (t + 1) * GROUP)
            copy = pltpu.make_async_copy(result.at[:, span], out_ref.at[:, span], sems.at[t // SPAN])
            copy.start()
            copies.append(copy)
    for copy in copies:
        copy.wait()


def swap(value, axis, size, bit):
    return lax.ppermute(value, axis, [(i, i ^ bit) for i in range(size)])


def turn_swap(value, rows, n_col, bits):
    turn = [
        (row * n_col + col, row * n_col + (col ^ bits[row % 2]))
        for row in range(rows)
        for col in range(n_col)
    ]
    return lax.ppermute(value, ("row", "col"), turn)


def send_order(chips):
    return sorted(range(1, chips), reverse=True)


def across_chips(pieces, rows):
    got = dict(pieces)
    for zs in send_order(rows // 2):
        if zs in pieces and zs != NEAR:
            got[zs] = swap(pieces[zs], "row", rows, 2 * zs)
    if NEAR in pieces:
        got[NEAR] = swap(pieces[NEAR], "row", rows, 2 * NEAR)
    return got


def on_device(mix_input, gate_logits, w_proj):
    return program(mix_input[0], gate_logits[0], w_proj)[None]


def program(tokens, gate, w_proj):
    count, features = tokens.shape
    rows, n_col = lax.axis_size("row"), lax.axis_size("col")
    chips = rows // 2
    lanes = features // (chips * CHUNKS)
    half = rows // 2
    width = w_proj.shape[1]
    scale = 1.0 / math.sqrt(count * rows * GROUP)
    table_hi, table_lo = split_halves(position_table(count, scale))
    narrow = jnp.asarray(twist_table(rows, count))
    features_of = feature_table(lanes // 2)
    feat = np.concatenate(split_halves(features_of), axis=1)
    bf = jnp.bfloat16
    fast = w_proj.shape[0] == GROUP and CHUNKS * lanes == GROUP and n_col == chips == 4

    half_w = jax.ShapeDtypeStruct((GROUP // 2, width), bf)
    picked = pl.pallas_call(
        functools.partial(pick_kernel, chips, fast),
        out_shape=[jax.ShapeDtypeStruct((count, lanes), bf)]
        + [jax.ShapeDtypeStruct((CHUNKS, count, lanes), bf)]
        + [jax.ShapeDtypeStruct((count, lanes), bf)] * (CHUNKS * (chips - 1) - 1)
        + [jax.ShapeDtypeStruct((count, rows), jnp.float32)]
        + [half_w] * (2 * fast),
        in_specs=[pl.BlockSpec(memory_space=pltpu.HBM)] * 3,
        out_specs=[pl.BlockSpec(memory_space=pltpu.VMEM)] * (CHUNKS * chips + 2 * fast),
        scratch_shapes=[
            pltpu.VMEM((count, features), bf),
            pltpu.SemaphoreType.DMA,
            pltpu.SemaphoreType.DMA((3,)),
        ],
        compiler_params=pltpu.CompilerParams(vmem_limit_bytes=24 * MIB),
        cost_estimate=pl.CostEstimate(
            flops=2 * count * GROUP * features, bytes_accessed=MIB, transcendentals=0
        ),
    )(*(pltpu.with_memory_space_constraint(v, pltpu.HBM) for v in (tokens, w_proj, narrow)))
    far = all_but_near(chips)
    first = across_chips(dict(enumerate(picked[:chips])), rows)
    second = across_chips(dict(zip(far, picked[chips:])), rows)
    arrived = [[first[zs] for zs in range(chips)]]
    arrived.append([{**second, NEAR: first[NEAR]}[zs] for zs in range(chips)])
    narrow_own, *halves = picked[2 * chips - 1 :]

    if fast:
        mine, rest = halves
        w_a = turn_swap(mine, rows, n_col, (1, 2))
        w_b = turn_swap(mine, rows, n_col, (2, 1))
        w_c = turn_swap(w_a, rows, n_col, (2, 1))
        others = []
        for own in (w_a, w_b, w_c):
            others.append(swap(own, "row", rows, 1))

    lines = half * (count // rows)
    piece = jax.ShapeDtypeStruct((2, lines, lanes), bf)
    small = (count * features // 4, count * features)

    def stacked(n):
        return jax.ShapeDtypeStruct((n, lines, lanes), bf)

    twist = vmem_call(
        twist_kernel, jax.ShapeDtypeStruct((rows, count, lanes), jnp.float32), [], *small
    )(narrow_own)
    line = jax.ShapeDtypeStruct((lines, lanes), bf)
    made = ([piece] * (chips - 1) + [line] * 2, [stacked(chips), stacked(chips + 1)])
    sent = []
    for q in range(CHUNKS):
        stack = vmem_call(
            functools.partial(stack_kernel, q),
            jax.ShapeDtypeStruct((chips, count, lanes), bf),
            [],
            *small,
        )(*arrived[q])
        theirs = swap(stack, "row", rows, 1)
        sent.append(
            vmem_call(
                functools.partial(position_kernel, rows, q),
                made[q],
                [
                    pltpu.VMEM((half, count, lanes), jnp.float32),
                    pltpu.VMEM((2 * count, half * lanes), bf),
                    pltpu.VMEM((half, count, lanes), jnp.float32),
                ],
                8 * count * count * half * lanes,
                rows * count * lanes * 4,
            )(*arrived[q], theirs, table_hi, table_lo, twist, *(sent[0][chips:] if q else ()))
        )
    early = across_chips(dict(zip(far, sent[0])), rows)
    early = [early[zs] for zs in far]
    give = vmem_call(give_kernel, stacked(chips - 1), [], *small)(*early)
    early.append(swap(give, "row", rows, 1))
    keep, give = sent[1]
    got = swap(give, "row", rows, 1)
    joined = vmem_call(
        join_kernel, [stacked(4 if zs == NEAR else 2) for zs in range(chips)], [], *small
    )(keep, got, sent[0][chips - 1])
    late = across_chips(dict(enumerate(joined)), rows)
    late = [late[zs] for zs in range(chips)]
    if fast:
        spect, opened = vmem_call(
            functools.partial(prepare_kernel, rows),
            [
                jax.ShapeDtypeStruct((chips, count, GROUP), jnp.float32),
                jax.ShapeDtypeStruct((count, width), jnp.float32),
            ],
            [],
            2 * count * features * GROUP,
            6 * count * width,
        )(*early, feat, gate)
        return pl.pallas_call(
            functools.partial(final_kernel, rows),
            out_shape=jax.ShapeDtypeStruct((count, width), bf),
            in_specs=[pl.BlockSpec(memory_space=pltpu.VMEM)] * (chips + 11),
            out_specs=pl.BlockSpec(memory_space=pl.ANY),
            scratch_shapes=[
                pltpu.VMEM((chips, count, GROUP), bf),
                pltpu.VMEM((count, width), bf),
                pltpu.SemaphoreType.DMA((width // GROUP,)),
            ],
            compiler_params=pltpu.CompilerParams(vmem_limit_bytes=32 * MIB),
            cost_estimate=pl.CostEstimate(
                flops=2 * count * features * width,
                bytes_accessed=2 * features * width,
                transcendentals=0,
            ),
        )(*late, feat, spect, opened, mine, rest, w_a, w_b, w_c, *others)

    weights = lax.all_gather(w_proj, "col", axis=0, tiled=True).reshape(-1, GROUP, width)
    order = order_rows(rows, count)
    chip = lax.axis_index("row") // 2
    table = jnp.asarray(features_of, jnp.float32).reshape(-1, CHUNKS, lanes, GROUP)
    per_group = table.shape[0]
    spectrum = jnp.zeros((count, weights.shape[0], GROUP), jnp.float32)
    here = chip ^ jnp.arange(chips)
    for q in range(CHUNKS):
        if q == 0:
            parts = [(early[i][0], early[-1][i]) for i in range(chips - 1)]
            parts.insert(NEAR, (late[NEAR][2], late[NEAR][3]))
        else:
            parts = [(ref[0], ref[1]) for ref in late]
        got = jnp.stack([jnp.concatenate(pair, axis=0) for pair in parts])[here]
        got = jnp.einsum("kr,zrl->kzl", order, got, preferred_element_type=jnp.float32)
        spectrum += jnp.einsum(
            "kgtl,tlm->kgm",
            got.reshape(count, -1, per_group, lanes),
            table[:, q],
            precision=lax.Precision.HIGHEST,
        )
    total = jnp.einsum(
        "kgm,gmd->kd", spectrum.astype(bf), weights, preferred_element_type=jnp.float32
    )
    return (jax.nn.sigmoid(gate.astype(jnp.float32)) * total).astype(bf)


def solution(mesh):
    spec = P("col", "row", None)
    return jax.shard_map(
        on_device, mesh=mesh, in_specs=(spec, spec, P("col", None)), out_specs=spec, check_vma=False
    )
```
